256 devices in a mesh: ep: 32 (over z, x), tp: 8 (over y, core).
Axes of the slice: x: 4, y: 4, z: 8, core: 2. Of those that a mesh axis runs over, the one named last changes fastest.
Arguments:
- tokens: bfloat16 [2048, 2048], P('ep', 'tp')
- norm_gain: float32 [2048], P('tp'), may hold values from 0.1 to 1.9
- expert_ids: int32 [2048, 4], P('ep'), may hold values from 0 to 31, all different within a row; in each aligned block of 64 rows (0 to 63, 64 to 127, ...) at most 16 rows name the same one
- route_weights: float32 [2048, 4], P('ep'), may hold values from 0.1 to 1
- gate_proj: bfloat16 [32, 2048, 2048], P('ep', None, 'tp'), may hold values from -0.5 to 0.5
- up_proj: bfloat16 [32, 2048, 2048], P('ep', None, 'tp'), may hold values from -0.5 to 0.5
- down_proj: bfloat16 [32, 2048, 2048], P('ep', 'tp')
- final_gain: float32 [2048], P('tp'), may hold values from 0.1 to 1.9
Outputs:
- layer_output: bfloat16 [2048, 2048], P('ep', 'tp')
The draws below stay inside these ranges and needn't reach their ends.
Inputs may be any that keep to these rules, and one draw needn't show every extreme that they name: `expert_ids`: each row names 4 different experts. Within the 64 rows of one device no expert is named by more than 16 rows, a bound that some block reaches.
All inputs are finite; a program needn't handle non-finite values.
Results may differ from the reference program's by a relative error of at most 0.017.
Values may be sent and summed in bfloat16 or wider, within the bound.
No kernel may reach another device: no remote copies, remote signals or barrier semaphores. Data moves between devices by JAX's collectives and lax.ppermute only.
A program may use at most 64 MiB of HBM per device.

```python
import math
import jax
import jax.numpy as jnp
import numpy as np
from jax import lax

D = 2048
FF = 2048
TOP_K = 4
TOK_DEV = 64
EXPERTS = 32
TOKENS = 2048
CAP = 16
N_EP = 32
N_TP = 8


def column_rise(count):
    return jnp.exp(math.log(6.0) * jnp.arange(count, dtype=jnp.float32) / (count - 1))


def draw_tokens(key, part):
    first_key, second_key = jax.random.split(key, 2)
    row_scales = jnp.exp(jax.random.uniform(second_key, (TOKENS, 1), jnp.float32, minval=math.log(0.3), maxval=math.log(3.0)))
    base = jax.random.normal(first_key, (TOKENS, D), jnp.float32)
    return (base * row_scales * column_rise(D)[None, :]).astype(jnp.bfloat16)


def draw_down_proj(key, part):
    first_key = jax.random.fold_in(key, 0)
    base = jax.random.normal(first_key, (EXPERTS, FF, D), jnp.float32)
    return (base * FF ** (-0.5) * column_rise(D)[None, None, :]).astype(jnp.bfloat16)


def shard_levels(key, extent, shards, low, top_value):
    def one(axis_at, blocks):
        steps = jax.random.uniform(jax.random.fold_in(jax.random.fold_in(key, 6), axis_at), (blocks,), jnp.float32, low / len(shards), top_value / len(shards))
        return jnp.repeat(jnp.exp(steps), extent[axis_at] // blocks).reshape((-1,) + (1,) * (len(extent) - axis_at - 1))

    gain = one(*shards[0])
    for cut in shards[1:]:
        gain = gain * one(*cut)
    return gain


def assign_block(own_key, own, number, rows, amount, top, most, skew):
    ranking = jax.random.permutation(own_key, amount)
    packed, ordinary = portions_of(amount, rows * top, most, skew, True), portions_of(amount, rows * top, most, skew, False)
    places = jnp.arange(amount)

    def named(lengths, turn):
        used = int((lengths > 0).sum())
        fixed = max(1, used // 4)
        moved = fixed + (places - fixed + turn * (used - fixed)) % max(1, amount - fixed)
        return jnp.zeros((amount,), jnp.int32).at[ranking[jnp.where(places < fixed, places, moved)]].set(jnp.asarray(lengths, jnp.int32))

    lengths = jnp.where(number % 4 == 0, named(packed, number // 4), named(ordinary, number - number // 4 - 1))
    mixed = jax.random.permutation(jax.random.fold_in(own, 3), amount)
    giver, sink = mixed[0:amount // 2 * 2:2], mixed[1:amount // 2 * 2:2]
    margin = jnp.minimum(lengths[giver] - 1, most - lengths[sink]) // 2
    margin = jnp.where((giver == ranking[0]) | (sink == ranking[0]) | (lengths[sink] == 0), 0, jnp.maximum(margin, 0))
    moved = jax.random.randint(jax.random.fold_in(own, 4), (amount // 2,), 0, 1 << 20) % (margin + 1)
    lengths = lengths.at[giver].add(-moved).at[sink].add(moved)
    labels = jnp.searchsorted(jnp.cumsum(lengths), jnp.arange(rows * top), side="right").astype(jnp.int32)
    table = labels.reshape(top, rows).T
    table = table[jax.random.permutation(jax.random.fold_in(own, 1), rows)]
    turn = jax.random.randint(jax.random.fold_in(own, 2), (rows, 1), 0, top)
    return jnp.take_along_axis(table, (jnp.arange(top)[None, :] + turn) % top, axis=1)


def portions_of(number_of, total, limit, skew, full):
    portions = [(1 << 20) // math.isqrt(rank ** skew) + 1 for rank in range(1, number_of + 1)]
    largest = limit if full else min(limit, max(-(-total // number_of), total * portions[0] // sum(portions)))
    least = 1 if total - largest >= number_of - 1 else 0
    counts, spare = [largest] + [least] * (number_of - 1), total - largest - least * (number_of - 1)
    while spare > 0:
        candidates = [i for i in range(1, number_of) if counts[i] < largest] or [i for i in range(1, number_of) if counts[i] < limit]
        pool, budget = sum([portions[i] for i in candidates]), spare
        for i in candidates:
            more = min(limit - counts[i], max(1, budget * portions[i] // pool), spare)
            counts[i] = counts[i] + more
            spare = spare - more
    return np.array(counts)


def normal_values(own_key, shape, scale, limit, cuts=(), kind=jnp.bfloat16):
    result = scale * jax.random.normal(own_key, shape, jnp.float32)
    if cuts:
        result = result * shard_levels(own_key, shape, cuts, -0.22, 0.18)
    return jnp.clip(result, -limit, limit).astype(kind)


def setup_inputs(seed: int = 0) -> dict:
    splits = jax.random.split(jax.random.key(seed), 9)
    tokens = draw_tokens(jax.random.fold_in(splits[8], 71), 0)
    norm_gain = jnp.clip(1.0 + 0.18 * jax.random.normal(splits[1], (D,), jnp.float32), 0.1, 1.9)
    expert_ids_keys = jax.random.split(jax.random.fold_in(splits[2], 1), TOKENS // TOK_DEV)
    expert_ids_turns = jax.random.permutation(jax.random.fold_in(splits[2], 3), TOKENS // TOK_DEV)
    expert_ids = jax.vmap(lambda own, number: assign_block(jax.random.fold_in(splits[2], 2), own, number, TOK_DEV, EXPERTS, TOP_K, CAP, 2))(expert_ids_keys, expert_ids_turns).reshape((TOKENS, TOP_K))
    route_weights = jnp.clip(0.1 + 0.9 * jax.random.uniform(splits[3], (TOKENS, TOP_K), jnp.float32) ** shard_levels(splits[3], (TOKENS, TOP_K), ((0, 32),), -0.2, 0.2), 0.1, 1.0)
    gate_proj = normal_values(splits[4], (EXPERTS, D, FF), (D // 16) ** -0.5, 0.5, ((0, 32), (2, 8)))
    up_proj = normal_values(splits[5], (EXPERTS, D, FF), (D // 16) ** -0.5, 0.5, ((0, 32), (2, 8)))
    down_proj = draw_down_proj(jax.random.fold_in(splits[8], 71), 0)
    final_gain = jnp.clip(1.0 + 0.18 * jax.random.normal(splits[7], (D,), jnp.float32), 0.1, 1.9)
    return {"tokens": tokens, "norm_gain": norm_gain, "expert_ids": expert_ids, "route_weights": route_weights, "gate_proj": gate_proj, "up_proj": up_proj, "down_proj": down_proj, "final_gain": final_gain}


EPSILON = 1e-05
CLAMP_LIMIT = 7.0
SIGMOID_SLOPE = 1.702

def slot_tables(id_block, gate_block, targets, capacity):
    matches = (id_block[:, :, None] == targets[None, None, :]).astype(jnp.int32)
    per_token = lax.optimization_barrier(jnp.sum(matches, axis=1))
    earlier = jnp.cumsum(per_token, axis=0) - per_token
    slot_places = lax.broadcasted_iota(jnp.int32, (1, 1, capacity), 2)
    selector = (per_token[:, :, None] * (earlier[:, :, None] == slot_places).astype(jnp.int32)).astype(jnp.float32)
    weights = lax.optimization_barrier(jnp.sum(gate_block[:, :, None] * matches.astype(jnp.float32), axis=1))
    return (selector, weights)

def reference(tokens, norm_gain, expert_ids, route_weights, gate_proj, up_proj, down_proj, final_gain):
    input_rows = tokens.astype(jnp.float32)
    row_scale = lax.rsqrt(lax.optimization_barrier(jnp.mean(input_rows * input_rows, axis=1, keepdims=True)) + EPSILON)
    normed = (input_rows * row_scale * norm_gain[None, :]).astype(jnp.bfloat16)
    targets = jnp.arange(EXPERTS, dtype=jnp.int32)

    def per_source(id_block, gate_block):
        return slot_tables(id_block, gate_block, targets, CAP)
    selector, weights = jax.vmap(per_source)(expert_ids.reshape(N_EP, TOK_DEV, TOP_K), route_weights.reshape(N_EP, TOK_DEV, TOP_K))
    blocks = normed.reshape(N_EP, TOK_DEV, D).astype(jnp.float32)
    select_by_expert = jnp.moveaxis(selector, 2, 0)
    weight_by_expert = jnp.moveaxis(weights, 2, 0)

    def one_expert(carry, inputs):
        chosen, gate_share, gate_w, up_w, down_w = inputs
        expert_rows = jnp.einsum('stc,std->scd', chosen, blocks).astype(jnp.bfloat16).reshape(-1, D)
        gate_pre = jnp.minimum(jnp.dot(expert_rows, gate_w, preferred_element_type=jnp.float32), CLAMP_LIMIT)
        up_pre = jnp.clip(jnp.dot(expert_rows, up_w, preferred_element_type=jnp.float32), -CLAMP_LIMIT, CLAMP_LIMIT)
        activated = ((up_pre + 1.0) * gate_pre * jax.nn.sigmoid(SIGMOID_SLOPE * gate_pre)).astype(jnp.bfloat16)
        partials = jnp.einsum('npf,pfd->npd', activated.reshape(-1, N_TP, FF // N_TP).astype(jnp.float32), down_w.reshape(N_TP, FF // N_TP, D).astype(jnp.float32))
        rounded = lax.optimization_barrier(partials.astype(jnp.bfloat16))
        expert_out = lax.optimization_barrier(jnp.sum(rounded.astype(jnp.float32), axis=1)).astype(jnp.bfloat16)
        contrib = jnp.einsum('stc,scd->std', chosen * gate_share[:, :, None], expert_out.astype(jnp.float32).reshape(N_EP, CAP, D))
        return (carry + contrib, None)
    summed, _ = lax.scan(one_expert, jnp.zeros((N_EP, TOK_DEV, D), jnp.float32), (select_by_expert, weight_by_expert, gate_proj, up_proj, down_proj))
    mixture = summed.reshape(TOKENS, D)
    out_scale = lax.rsqrt(lax.optimization_barrier(jnp.mean(mixture * mixture, axis=1, keepdims=True)) + EPSILON)
    return (mixture * out_scale * final_gain[None, :]).astype(jnp.bfloat16)
```

```python
import functools

import jax
import jax.numpy as jnp
from jax import lax
from jax.experimental import pallas as pl
from jax.experimental.pallas import tpu as pltpu
from jax.sharding import PartitionSpec as P

EPSILON = 1e-05
CLAMP_LIMIT = 7.0
SIGMOID_SLOPE = 1.702
CORES = 2
TAIL = 16
VMEM = pl.BlockSpec(memory_space=pltpu.VMEM)
SMEM = pl.BlockSpec(memory_space=pltpu.SMEM)


def split3(v):
    hi = v.astype(jnp.bfloat16)
    rest = v - hi.astype(jnp.float32)
    mid = rest.astype(jnp.bfloat16)
    lo = (rest - mid.astype(jnp.float32)).astype(jnp.bfloat16)
    return hi, mid, lo


def dot_t(a, b):
    return lax.dot_general(a, b, (((1,), (1,)), ((), ())), preferred_element_type=jnp.float32)


def dot_0(a, b):
    return lax.dot_general(a, b, (((0,), (0,)), ((), ())), preferred_element_type=jnp.float32)


def slot_matrix(ids, experts, capacity):
    choices, tokens = ids.shape
    expert = lax.broadcasted_iota(jnp.int32, (experts, tokens), 0)
    named = [(ids[k : k + 1, :] == expert).astype(jnp.float32) for k in range(choices)]
    match = functools.reduce(jnp.add, named)
    before = lax.broadcasted_iota(jnp.int32, (tokens, tokens), 0)
    after = lax.broadcasted_iota(jnp.int32, (tokens, tokens), 1)
    earlier = (before < after).astype(jnp.bfloat16)
    place = jnp.dot(match.astype(jnp.bfloat16), earlier, preferred_element_type=jnp.float32)
    place = jnp.where(match > 0.0, place, -1.0)

    def spread(rows):
        wide = jnp.broadcast_to(rows[:, None, :], (experts, capacity, tokens))
        return wide.reshape(experts * capacity, tokens)

    slot = lax.broadcasted_iota(jnp.int32, (experts, capacity, tokens), 1)
    slot = slot.reshape(experts * capacity, tokens).astype(jnp.float32)
    holds = spread(place) == slot
    return holds, named, spread


def pick_kernel(experts, capacity, ids_ref, tokens_ref, rows_ref):
    holds, _, _ = slot_matrix(ids_ref[...], experts, capacity)
    picked = jnp.dot(
        holds.astype(jnp.bfloat16), tokens_ref[...], preferred_element_type=jnp.float32
    )
    rows_ref[...] = picked.astype(jnp.bfloat16)


def mid_kernel(rows_ref, gain_ref, out_ref):
    rows = rows_ref.shape[0]
    x = rows_ref[...].astype(jnp.float32)
    out_ref[0:rows, :] = (x * gain_ref[...]).astype(jnp.bfloat16)
    sq = x * x
    hi, mid, _ = split3(sq)
    ones = jnp.ones((8, x.shape[1]), jnp.bfloat16)
    sums = dot_t(ones, hi) + dot_t(ones, mid)
    width = x.shape[1]
    row = lax.broadcasted_iota(jnp.int32, (8, width), 0)
    for part in range(rows // width):
        hi, mid, lo = split3(sums[:, part * width : (part + 1) * width])
        pieces = jnp.where(
            row == 0,
            hi.astype(jnp.float32),
            jnp.where(row == 1, mid.astype(jnp.float32), lo.astype(jnp.float32)),
        )
        pieces = jnp.where(row < 3, pieces, 0.0)
        tail = jnp.concatenate([pieces, jnp.zeros_like(pieces)], axis=0)
        out_ref[rows + part * TAIL : rows + (part + 1) * TAIL, :] = tail.astype(jnp.bfloat16)


def place(step, other, chips):
    me = lax.axis_index("tp")
    return (me // CORES + step + chips) % chips * CORES + (me % CORES + other) % CORES


def up_kernel(places, *refs):
    pieces = refs[:8]
    gate_ref, up_ref, act_ref = refs[8:]
    rows = act_ref.shape[0]
    width = pieces[0].shape[1]
    model_width = gate_ref.shape[0]
    ones = jnp.ones((TAIL, 128), jnp.bfloat16)
    for part in range(rows // width):
        at = part * width
        gate = jnp.zeros((width, width), jnp.float32)
        up = jnp.zeros((width, width), jnp.float32)
        squares = jnp.zeros((width, 128), jnp.float32)
        for i, piece in enumerate(pieces):
            from_row = pl.ds(pl.multiple_of(place(*places[i]) * width, width), width)
            x = piece[at : at + width, :]
            gate += jnp.dot(x, gate_ref[from_row, :], preferred_element_type=jnp.float32)
            up += jnp.dot(x, up_ref[from_row, :], preferred_element_type=jnp.float32)
            squares += dot_0(piece[rows + part * TAIL : rows + (part + 1) * TAIL, :], ones)
        scale = lax.rsqrt(squares / model_width + EPSILON)
        scale = jnp.concatenate([scale] * (width // 128), axis=1)
        gate = jnp.minimum(gate * scale, CLAMP_LIMIT)
        up = jnp.clip(up * scale, -CLAMP_LIMIT, CLAMP_LIMIT)
        act = (up + 1.0) * gate * jax.nn.sigmoid(SIGMOID_SLOPE * gate)
        act_ref[at : at + width, :] = act.astype(jnp.bfloat16)


def down_kernel(places, own_ref, other_ref, down_ref, down_other_ref, *outs):
    width = own_ref.shape[1]
    for i, out in enumerate(outs):
        columns = pl.ds(pl.multiple_of(place(*places[i]) * width, width), width)
        total = jnp.dot(own_ref[...], down_ref[:, columns], preferred_element_type=jnp.float32)
        total += jnp.dot(
            other_ref[...], down_other_ref[:, columns], preferred_element_type=jnp.float32
        )
        out[...] = total.astype(jnp.bfloat16)


def combine_kernel(experts, capacity, ids_ref, weights_ref, rows_ref, mix_ref, squares_ref):
    holds, named, spread = slot_matrix(ids_ref[...], experts, capacity)
    weights = weights_ref[...]
    share = functools.reduce(
        jnp.add, [weights[k : k + 1, :] * named[k] for k in range(len(named))]
    )
    share = jnp.where(holds, spread(share), 0.0)
    rows = rows_ref[...]
    mix = functools.reduce(jnp.add, [dot_0(part, rows) for part in split3(share)])
    mix_ref[...] = mix
    ones = jnp.ones((8, mix.shape[1]), jnp.bfloat16)
    sums = functools.reduce(jnp.add, [dot_t(ones, part) for part in split3(mix * mix)])
    sums = jnp.concatenate([sums, jnp.zeros_like(sums)], axis=1)
    for i in range(squares_ref.shape[0]):
        squares_ref[i] = sums


def final_kernel(model_width, mix_ref, squares_ref, gain_ref, out_ref):
    total = squares_ref[0]
    for i in range(1, squares_ref.shape[0]):
        total += squares_ref[i]
    mix = mix_ref[...]
    tokens = mix.shape[0]
    wide = jnp.concatenate([total] * (tokens // 8), axis=0)
    row = lax.broadcasted_iota(jnp.int32, wide.shape, 0)
    lane = lax.broadcasted_iota(jnp.int32, wide.shape, 1)
    column = jnp.sum(jnp.where(row == lane, wide, 0.0), axis=1, keepdims=True)
    scale = lax.rsqrt(column / model_width + EPSILON)
    out_ref[...] = (mix * scale * gain_ref[...]).astype(jnp.bfloat16)


def call(kernel, outs, *args, smem=0, limit=8):
    single = not isinstance(outs, (list, tuple))
    specs = [SMEM] * smem + [VMEM] * (len(args) - smem)
    return pl.pallas_call(
        kernel,
        out_shape=outs,
        in_specs=specs,
        out_specs=VMEM if single else [VMEM] * len(outs),
        compiler_params=pltpu.CompilerParams(vmem_limit_bytes=limit << 20),
    )(*args)


def shape_of(dims, dtype):
    return jax.ShapeDtypeStruct(dims, dtype)


def local(tokens, norm_gain, expert_ids, route_weights, gate_proj, up_proj, down_proj, final_gain):
    tok_rows, width = tokens.shape
    peers = lax.axis_size("tp")
    experts = lax.axis_size("ep")
    chips = peers // CORES
    capacity = min(tok_rows, 2 * tok_rows * expert_ids.shape[1] // experts)
    rows = experts * capacity
    model_width = width * peers

    def along(value, step):
        pairs = [
            (y * CORES + c, ((y + step) % chips) * CORES + c)
            for y in range(chips)
            for c in range(CORES)
        ]
        return lax.ppermute(value, "tp", pairs)

    def swap(value):
        pairs = [(y * CORES + c, y * CORES + 1 - c) for y in range(chips) for c in range(CORES)]
        return lax.ppermute(value, "tp", pairs)

    ids = expert_ids.T
    weights = route_weights.T
    down_other = swap(down_proj[0])

    outbound = call(
        functools.partial(pick_kernel, experts, capacity),
        shape_of((rows, width), jnp.bfloat16),
        ids,
        tokens,
    )
    received = lax.all_to_all(
        outbound.reshape(experts, capacity, width), "ep", split_axis=0, concat_axis=0, tiled=True
    ).reshape(rows, width)
    piece = call(
        mid_kernel,
        shape_of((rows + rows // width * TAIL, width), jnp.bfloat16),
        received,
        norm_gain[None, :],
    )
    offsets = [0, 1, chips - 1, 2]
    by_chip = [piece] + [along(piece, step) for step in offsets[1:]]
    pieces, places = [], []
    for step, held in zip(offsets, by_chip):
        pieces += [held, swap(held)]
        places += [(-step, 0, chips), (-step, 1, chips)]
    act = call(
        functools.partial(up_kernel, places),
        shape_of((rows, width), jnp.bfloat16),
        *pieces,
        gate_proj[0],
        up_proj[0],
        limit=16,
    )
    act_other = swap(act)
    chunks = call(
        functools.partial(down_kernel, [(step, 0, chips) for step in offsets]),
        [shape_of((rows, width), jnp.bfloat16)] * chips,
        act,
        act_other,
        down_proj[0],
        down_other,
        limit=16,
    )
    arrived = [chunks[0]] + [along(chunk, step) for chunk, step in zip(chunks[1:], offsets[1:])]
    total = functools.reduce(jnp.add, [part.astype(jnp.float32) for part in arrived])
    expert_out = total.astype(jnp.bfloat16).reshape(experts, capacity, width)
    returned = lax.all_to_all(expert_out, "ep", split_axis=0, concat_axis=0, tiled=True)
    mixture, squares = call(
        functools.partial(combine_kernel, experts, capacity),
        [shape_of((tok_rows, width), jnp.float32), shape_of((peers, 8, 128), jnp.float32)],
        ids,
        weights,
        returned.reshape(rows, width),
    )
    squares = lax.all_to_all(squares, "tp", split_axis=0, concat_axis=0, tiled=True)
    return call(
        functools.partial(final_kernel, model_width),
        shape_of((tok_rows, width), jnp.bfloat16),
        mixture,
        squares,
        final_gain[None, :],
    )


def solution(mesh):
    placed = (
        P("ep", "tp"),
        P("tp"),
        P("ep", None),
        P("ep", None),
        P("ep", None, "tp"),
        P("ep", None, "tp"),
        P("ep", "tp", None),
        P("tp"),
    )
    return jax.shard_map(
        local, mesh=mesh, in_specs=placed, out_specs=P("ep", "tp"), check_vma=False
    )
```

```python
import functools

import jax
import jax.numpy as jnp
from jax import lax
from jax.experimental import pallas as pl
from jax.experimental.pallas import tpu as pltpu
from jax.sharding import PartitionSpec as P


EPSILON = 1e-05
CLAMP_LIMIT = 7.0
SIGMOID_SLOPE = 1.702
CORES = 2
TAIL = 16
VMEM = pl.BlockSpec(memory_space=pltpu.VMEM)
HBM = pl.BlockSpec(memory_space=pltpu.HBM)


def split3(v):
    hi = v.astype(jnp.bfloat16)
    rest = v - hi.astype(jnp.float32)
    mid = rest.astype(jnp.bfloat16)
    lo = (rest - mid.astype(jnp.float32)).astype(jnp.bfloat16)
    return hi, mid, lo


def dot_t(a, b):
    return lax.dot_general(a, b, (((1,), (1,)), ((), ())), preferred_element_type=jnp.float32)


def dot_0(a, b):
    return lax.dot_general(a, b, (((0,), (0,)), ((), ())), preferred_element_type=jnp.float32)


def slot_matrix(ids, experts, capacity):
    choices, tokens = ids.shape
    expert = lax.broadcasted_iota(jnp.int32, (experts, tokens), 0)
    named = [(ids[k : k + 1, :] == expert).astype(jnp.float32) for k in range(choices)]
    match = functools.reduce(jnp.add, named)
    before = lax.broadcasted_iota(jnp.int32, (tokens, tokens), 0)
    after = lax.broadcasted_iota(jnp.int32, (tokens, tokens), 1)
    earlier = (before < after).astype(jnp.bfloat16)
    place = jnp.dot(match.astype(jnp.bfloat16), earlier, preferred_element_type=jnp.float32)
    place = jnp.where(match > 0.0, place, -1.0)

    def spread(rows):
        wide = jnp.broadcast_to(rows[:, None, :], (experts, capacity, tokens))
        return wide.reshape(experts * capacity, tokens)

    slot = lax.broadcasted_iota(jnp.int32, (experts, capacity, tokens), 1)
    slot = slot.reshape(experts * capacity, tokens).astype(jnp.float32)
    holds = spread(place) == slot
    return holds, named, spread


def pick_kernel(experts, capacity, ids_hbm, tokens_hbm, gain_hbm, rows_ref, gain_ref, ids_ref, tokens_ref, sems):
    copies = [
        pltpu.make_async_copy(ids_hbm, ids_ref, sems.at[0]),
        pltpu.make_async_copy(tokens_hbm, tokens_ref, sems.at[1]),
        pltpu.make_async_copy(gain_hbm, gain_ref, sems.at[2]),
    ]
    for copy in copies:
        copy.start()
    copies[0].wait()
    holds, _, _ = slot_matrix(ids_ref[...], experts, capacity)
    holds = holds.astype(jnp.bfloat16)
    copies[1].wait()
    picked = jnp.dot(holds, tokens_ref[...], preferred_element_type=jnp.float32)
    rows_ref[...] = picked.astype(jnp.bfloat16)
    copies[2].wait()


def load_kernel(experts, capacity, *refs):
    ids_hbm, weights_hbm, *sources = refs[:6]
    share_ref, *targets = refs[6:11]
    ids_ref, weights_ref, sems = refs[11:]
    pairs = [(ids_hbm, ids_ref), (weights_hbm, weights_ref), *zip(sources, targets)]
    copies = [pltpu.make_async_copy(*pair, sems.at[i]) for i, pair in enumerate(pairs)]
    for copy in copies:
        copy.start()
    copies[0].wait()
    holds, named, spread = slot_matrix(ids_ref[...], experts, capacity)
    copies[1].wait()
    weights = weights_ref[...]
    share = functools.reduce(
        jnp.add, [weights[k : k + 1, :] * named[k] for k in range(len(named))]
    )
    share = jnp.where(holds, spread(share), 0.0).T
    tokens = share.shape[0]
    for i, part in enumerate(split3(share)):
        share_ref[i * tokens : (i + 1) * tokens, :] = part
    for copy in copies[2:]:
        copy.wait()


def mid_kernel(rows_ref, gain_ref, out_ref):
    rows, width = rows_ref.shape
    x = rows_ref[...].astype(jnp.float32)
    out_ref[0:rows, :] = (x * gain_ref[...]).astype(jnp.bfloat16)
    hi, mid, _ = split3(x * x)
    ones = jnp.ones((8, width), jnp.bfloat16)
    sums = dot_t(ones, hi) + dot_t(ones, mid)
    row = lax.broadcasted_iota(jnp.int32, (8, width), 0)
    tail = []
    for part in range(rows // width):
        pieces = [v.astype(jnp.float32) for v in split3(sums[:, part * width : (part + 1) * width])]
        tail.append(
            jnp.where(
                row == 0,
                pieces[0],
                jnp.where(row == 1, pieces[1], jnp.where(row == 2, pieces[2], 0.0)),
            )
        )
    out_ref[rows : rows + TAIL, :] = jnp.concatenate(tail, axis=0).astype(jnp.bfloat16)


def ahead(step, other, chips):
    me = lax.axis_index("tp")
    core = me % CORES
    return (me // CORES + step * (1 - 2 * core) + chips) % chips * CORES + (core + other) % CORES


def products(part, width, places, pieces, gate_ref, up_ref, gate, up, squares):
    rows = pieces[0].shape[0] - TAIL
    at = part * width
    row = lax.broadcasted_iota(jnp.int32, (TAIL, 128), 0)
    ones = jnp.where(row // 8 == part, 1.0, 0.0).astype(jnp.bfloat16)
    for where, piece in zip(places, pieces):
        from_row = pl.ds(pl.multiple_of(ahead(*where) * width, width), width)
        x = piece[at : at + width, :]
        gate += jnp.dot(x, gate_ref[from_row, :], preferred_element_type=jnp.float32)
        up += jnp.dot(x, up_ref[from_row, :], preferred_element_type=jnp.float32)
        squares += dot_0(piece[rows : rows + TAIL, :], ones)
    return gate, up, squares


def first_kernel(places, *refs):
    count = len(places)
    gate_ref, up_ref, gate_out, up_out, squares_out = refs[count:]
    width = gate_ref.shape[1]
    for part in range(gate_out.shape[0] // width):
        at = slice(part * width, (part + 1) * width)
        zero = jnp.zeros((width, width), jnp.float32)
        gate, up, squares = products(
            part, width, places, refs[:count], gate_ref, up_ref, zero, zero, zero[:, :128]
        )
        gate_out[at, :] = gate
        up_out[at, :] = up
        squares_out[at, :] = squares


def last_kernel(places, *refs):
    count = len(places)
    gate_ref, up_ref, gate_in, up_in, squares_in, act_ref = refs[count:]
    model_width, width = gate_ref.shape
    for part in range(gate_in.shape[0] // width):
        at = slice(part * width, (part + 1) * width)
        gate, up, squares = products(
            part, width, places, refs[:count], gate_ref, up_ref,
            gate_in[at, :], up_in[at, :], squares_in[at, :],
        )
        scale = lax.rsqrt(squares / model_width + EPSILON)
        scale = jnp.concatenate([scale] * (width // 128), axis=1)
        gate = jnp.minimum(gate * scale, CLAMP_LIMIT)
        up = jnp.clip(up * scale, -CLAMP_LIMIT, CLAMP_LIMIT)
        act = (up + 1.0) * gate * jax.nn.sigmoid(SIGMOID_SLOPE * gate)
        act_ref[at, :] = act.astype(jnp.bfloat16)


def down_kernel(places, own_ref, other_ref, down_ref, down_other_ref, *outs):
    width = own_ref.shape[1]
    for where, out in zip(places, outs):
        columns = pl.ds(pl.multiple_of(ahead(*where) * width, width), width)
        total = jnp.dot(own_ref[...], down_ref[:, columns], preferred_element_type=jnp.float32)
        total += jnp.dot(
            other_ref[...], down_other_ref[:, columns], preferred_element_type=jnp.float32
        )
        out[...] = total.astype(jnp.bfloat16)


def combine_kernel(share_ref, rows_ref, mix_ref, squares_ref):
    tokens = mix_ref.shape[0]
    parts = jnp.dot(share_ref[...], rows_ref[...], preferred_element_type=jnp.float32)
    mix = parts[:tokens] + parts[tokens : 2 * tokens] + parts[2 * tokens :]
    mix_ref[...] = mix
    ones = jnp.ones((8, mix.shape[1]), jnp.bfloat16)
    sums = functools.reduce(jnp.add, [dot_t(ones, part) for part in split3(mix * mix)])
    sums = jnp.concatenate([sums, jnp.zeros_like(sums)], axis=1)
    for i in range(squares_ref.shape[0]):
        squares_ref[i] = sums


def final_kernel(model_width, mix_ref, squares_ref, gain_ref, out_ref):
    total = squares_ref[0]
    for i in range(1, squares_ref.shape[0]):
        total += squares_ref[i]
    mix = mix_ref[...]
    tokens = mix.shape[0]
    wide = jnp.concatenate([total] * (tokens // 8), axis=0)
    row = lax.broadcasted_iota(jnp.int32, wide.shape, 0)
    lane = lax.broadcasted_iota(jnp.int32, wide.shape, 1)
    column = jnp.sum(jnp.where(row == lane, wide, 0.0), axis=1, keepdims=True)
    scale = lax.rsqrt(column / model_width + EPSILON)
    out_ref[...] = (mix * scale * gain_ref[...]).astype(jnp.bfloat16)


def call(kernel, outs, *args, limit=8, flops=0, space=VMEM, scratch=()):
    single = not isinstance(outs, (list, tuple))
    if space is HBM:
        args = [pltpu.with_memory_space_constraint(arg, pltpu.HBM) for arg in args]
    return pl.pallas_call(
        kernel,
        out_shape=outs,
        in_specs=[space] * len(args),
        out_specs=VMEM if single else [VMEM] * len(outs),
        scratch_shapes=scratch,
        cost_estimate=pl.CostEstimate(flops=flops, bytes_accessed=0, transcendentals=0),
        compiler_params=pltpu.CompilerParams(vmem_limit_bytes=limit << 20),
    )(*args)


def shape_of(dims, dtype):
    return jax.ShapeDtypeStruct(dims, dtype)


def local(tokens, norm_gain, expert_ids, route_weights, gate_proj, up_proj, down_proj, final_gain):
    tok_rows, width = tokens.shape
    peers = lax.axis_size("tp")
    experts = lax.axis_size("ep")
    chips = peers // CORES
    capacity = min(tok_rows, 2 * tok_rows * expert_ids.shape[1] // experts)
    rows = experts * capacity
    model_width = width * peers

    def onward(value):
        pairs = [
            (y * CORES + c, ((y + 1 - 2 * c) % chips) * CORES + c)
            for y in range(chips)
            for c in range(CORES)
        ]
        return lax.ppermute(value, "tp", pairs)

    def swap(value):
        pairs = [(y * CORES + c, y * CORES + 1 - c) for y in range(chips) for c in range(CORES)]
        return lax.ppermute(value, "tp", pairs)

    narrow = shape_of((rows, width), jnp.bfloat16)
    ids = expert_ids.T
    outbound, gain = call(
        functools.partial(pick_kernel, experts, capacity),
        [narrow, shape_of((1, width), jnp.float32)],
        ids,
        tokens,
        norm_gain[None, :],
        space=HBM,
        scratch=(
            pltpu.VMEM(ids.shape, jnp.int32),
            pltpu.VMEM(tokens.shape, jnp.bfloat16),
            pltpu.SemaphoreType.DMA((3,)),
        ),
    )
    received = lax.all_to_all(
        outbound.reshape(experts, capacity, width), "ep", split_axis=0, concat_axis=0, tiled=True
    ).reshape(rows, width)
    own = call(mid_kernel, shape_of((rows + TAIL, width), jnp.bfloat16), received, gain)

    first = onward(own)
    own_other = swap(own)
    sources = (ids, route_weights.T, final_gain[None, :], gate_proj[0], up_proj[0], down_proj[0])
    share, final_gain, gate, up, down = call(
        functools.partial(load_kernel, experts, capacity),
        [shape_of((3 * tok_rows, rows), jnp.bfloat16)]
        + [shape_of(source.shape, source.dtype) for source in sources[2:]],
        *sources,
        space=HBM,
        scratch=(
            pltpu.VMEM(ids.shape, jnp.int32),
            pltpu.VMEM(ids.shape, jnp.float32),
            pltpu.SemaphoreType.DMA((len(sources),)),
        ),
    )
    down_other = swap(down)
    second = onward(own_other)
    third = onward(first)
    first_other = swap(first)
    second_other = swap(second)
    third_other = swap(third)
    held = [
        (own, (0, 0)),
        (own_other, (0, 1)),
        (first, (-1, 0)),
        (first_other, (1, 1)),
        (second, (-1, 1)),
        (second_other, (1, 0)),
        (third, (-2, 0)),
        (third_other, (2, 1)),
    ]
    places = [where + (chips,) for _, where in held]
    early = 6
    wide = shape_of((rows, width), jnp.float32)
    flops = 4 * rows * width * width
    sums = call(
        functools.partial(first_kernel, places[:early]),
        [wide, wide, shape_of((rows, 128), jnp.float32)],
        *[piece for piece, _ in held[:early]],
        gate,
        up,
        limit=16,
        flops=early * flops,
    )
    act = call(
        functools.partial(last_kernel, places[early:]),
        narrow,
        *[piece for piece, _ in held[early:]],
        gate,
        up,
        *sums,
        limit=16,
        flops=(len(held) - early) * flops,
    )
    act_other = swap(act)
    wanted = [(2, 0, chips), (1, 1, chips), (1, 0, chips), (0, 0, chips)]
    far, near_other, near, kept = call(
        functools.partial(down_kernel, wanted),
        [narrow] * len(wanted),
        act,
        act_other,
        down,
        down_other,
        limit=16,
        flops=len(wanted) * flops,
    )
    far = onward(far)
    near_other = swap(onward(near_other))
    near = (near.astype(jnp.float32) + far.astype(jnp.float32)).astype(jnp.bfloat16)
    near = onward(near)
    total = functools.reduce(
        jnp.add, [part.astype(jnp.float32) for part in (kept, near_other, near)]
    )
    expert_out = total.astype(jnp.bfloat16).reshape(experts, capacity, width)
    returned = lax.all_to_all(expert_out, "ep", split_axis=0, concat_axis=0, tiled=True)
    mixture, squares = call(
        combine_kernel,
        [shape_of((tok_rows, width), jnp.float32), shape_of((peers, 8, 128), jnp.float32)],
        share,
        returned.reshape(rows, width),
    )
    squares = lax.all_to_all(squares, "tp", split_axis=0, concat_axis=0, tiled=True)
    return call(
        functools.partial(final_kernel, model_width),
        shape_of((tok_rows, width), jnp.bfloat16),
        mixture,
        squares,
        final_gain,
    )


def solution(mesh):
    placed = (
        P("ep", "tp"),
        P("tp"),
        P("ep", None),
        P("ep", None),
        P("ep", None, "tp"),
        P("ep", None, "tp"),
        P("ep", "tp", None),
        P("tp"),
    )

    return jax.shard_map(
        local, mesh=mesh, in_specs=placed, out_specs=P("ep", "tp"), check_vma=False
    )
```

```python
import functools

import jax
import jax.numpy as jnp
from jax import lax
from jax.experimental import pallas as pl
from jax.experimental.pallas import tpu as pltpu
from jax.sharding import PartitionSpec as P


EPSILON = 1e-05
CLAMP_LIMIT = 7.0
SIGMOID_SLOPE = 1.702
CORES = 2
TAIL = 16
VMEM = pl.BlockSpec(memory_space=pltpu.VMEM)
HBM = pl.BlockSpec(memory_space=pltpu.HBM)


def split3(v):
    hi = v.astype(jnp.bfloat16)
    rest = v - hi.astype(jnp.float32)
    mid = rest.astype(jnp.bfloat16)
    lo = (rest - mid.astype(jnp.float32)).astype(jnp.bfloat16)
    return hi, mid, lo


def dot_t(a, b):
    return lax.dot_general(a, b, (((1,), (1,)), ((), ())), preferred_element_type=jnp.float32)


def dot_0(a, b):
    return lax.dot_general(a, b, (((0,), (0,)), ((), ())), preferred_element_type=jnp.float32)


def slot_matrix(ids, experts, capacity):
    choices, tokens = ids.shape
    expert = lax.broadcasted_iota(jnp.int32, (experts, tokens), 0)
    named = [(ids[k : k + 1, :] == expert).astype(jnp.float32) for k in range(choices)]
    match = functools.reduce(jnp.add, named)
    before = lax.broadcasted_iota(jnp.int32, (tokens, tokens), 0)
    after = lax.broadcasted_iota(jnp.int32, (tokens, tokens), 1)
    earlier = (before < after).astype(jnp.bfloat16)
    place = jnp.dot(match.astype(jnp.bfloat16), earlier, preferred_element_type=jnp.float32)
    place = jnp.where(match > 0.0, place, -1.0)

    def spread(rows):
        wide = jnp.broadcast_to(rows[:, None, :], (experts, capacity, tokens))
        return wide.reshape(experts * capacity, tokens)

    slot = lax.broadcasted_iota(jnp.int32, (experts, capacity, tokens), 1)
    slot = slot.reshape(experts * capacity, tokens).astype(jnp.float32)
    holds = spread(place) == slot
    return holds, named, spread


def pick_kernel(experts, capacity, ids_hbm, tokens_hbm, gain_hbm, rows_ref, gain_ref, ids_ref, tokens_ref, sems):
    copies = [
        pltpu.make_async_copy(ids_hbm, ids_ref, sems.at[0]),
        pltpu.make_async_copy(tokens_hbm, tokens_ref, sems.at[1]),
        pltpu.make_async_copy(gain_hbm, gain_ref, sems.at[2]),
    ]
    for copy in copies:
        copy.start()
    copies[0].wait()
    holds, _, _ = slot_matrix(ids_ref[...], experts, capacity)
    holds = holds.astype(jnp.bfloat16)
    copies[1].wait()
    picked = jnp.dot(holds, tokens_ref[...], preferred_element_type=jnp.float32)
    rows_ref[...] = picked.astype(jnp.bfloat16)
    copies[2].wait()


def load_kernel(experts, capacity, *refs):
    *refs, ids_ref, weights_ref, sems = refs
    count = (len(refs) + 1) // 2
    ids_hbm, weights_hbm, *sources = refs[:count]
    share_ref, *targets = refs[count:]
    pairs = [(ids_hbm, ids_ref), (weights_hbm, weights_ref), *zip(sources, targets)]
    copies = [pltpu.make_async_copy(*pair, sems.at[i]) for i, pair in enumerate(pairs)]
    for copy in copies:
        copy.start()
    copies[0].wait()
    holds, named, spread = slot_matrix(ids_ref[...], experts, capacity)
    copies[1].wait()
    weights = weights_ref[...]
    share = functools.reduce(
        jnp.add, [weights[k : k + 1, :] * named[k] for k in range(len(named))]
    )
    share = jnp.where(holds, spread(share), 0.0).T
    tokens = share.shape[0]
    for i, part in enumerate(split3(share)):
        share_ref[i * tokens : (i + 1) * tokens, :] = part
    for copy in copies[2:]:
        copy.wait()


def mid_kernel(rows_ref, gain_ref, out_ref, out_a_ref, out_b_ref):
    rows, width = rows_ref.shape
    half = rows // 2
    x = rows_ref[...].astype(jnp.float32)
    scaled = (x * gain_ref[...]).astype(jnp.bfloat16)
    out_ref[0:rows, :] = scaled
    out_a_ref[0:half, :] = scaled[:half]
    out_b_ref[...] = scaled[half:]
    hi, mid, _ = split3(x * x)
    ones = jnp.ones((8, width), jnp.bfloat16)
    sums = dot_t(ones, hi) + dot_t(ones, mid)
    row = lax.broadcasted_iota(jnp.int32, (8, width), 0)
    tail = []
    for part in range(rows // width):
        pieces = [v.astype(jnp.float32) for v in split3(sums[:, part * width : (part + 1) * width])]
        tail.append(
            jnp.where(
                row == 0,
                pieces[0],
                jnp.where(row == 1, pieces[1], jnp.where(row == 2, pieces[2], 0.0)),
            )
        )
    tail = jnp.concatenate(tail, axis=0).astype(jnp.bfloat16)
    out_ref[rows : rows + TAIL, :] = tail
    out_a_ref[half : half + TAIL, :] = tail


def ahead(step, other, chips):
    me = lax.axis_index("tp")
    core = me % CORES
    return (me // CORES + step * (1 - 2 * core) + chips) % chips * CORES + (core + other) % CORES


def products(part, pieces, gate_ref, up_ref, gate, up, squares):
    width = gate_ref.shape[1]
    row = lax.broadcasted_iota(jnp.int32, (TAIL, 128), 0)
    ones = jnp.where(row // 8 == part, 1.0, 0.0).astype(jnp.bfloat16)
    for where, refs in pieces:
        from_row = pl.ds(pl.multiple_of(ahead(*where) * width, width), width)
        at = part * width if len(refs) == 1 else 0
        x = refs[part if len(refs) > 1 else 0][at : at + width, :]
        end = refs[0].shape[0]
        gate += jnp.dot(x, gate_ref[from_row, :], preferred_element_type=jnp.float32)
        up += jnp.dot(x, up_ref[from_row, :], preferred_element_type=jnp.float32)
        squares += dot_0(refs[0][end - TAIL : end, :], ones)
    return gate, up, squares


def grouped(places, sizes, refs):
    pieces, at = [], 0
    for where, size in zip(places, sizes):
        pieces.append((where, refs[at : at + size]))
        at += size
    return pieces, refs[at:]


def first_kernel(places, sizes, *refs):
    pieces, (gate_ref, up_ref, gate_out, up_out, squares_out) = grouped(places, sizes, refs)
    width = gate_ref.shape[1]
    for part in range(gate_out.shape[0] // width):
        at = slice(part * width, (part + 1) * width)
        zero = jnp.zeros((width, width), jnp.float32)
        gate, up, squares = products(part, pieces, gate_ref, up_ref, zero, zero, zero[:, :128])
        gate_out[at, :] = gate
        up_out[at, :] = up
        squares_out[at, :] = squares


def last_kernel(places, sizes, part, *refs):
    pieces, refs = grouped(places, sizes, refs)
    gate_ref, up_ref, gate_in, up_in, squares_in, act_ref = refs
    model_width, width = gate_ref.shape
    at = slice(part * width, (part + 1) * width)
    gate, up, squares = products(
        part, pieces, gate_ref, up_ref, gate_in[at, :], up_in[at, :], squares_in[at, :]
    )
    scale = lax.rsqrt(squares / model_width + EPSILON)
    scale = jnp.concatenate([scale] * (width // 128), axis=1)
    gate = jnp.minimum(gate * scale, CLAMP_LIMIT)
    up = jnp.clip(up * scale, -CLAMP_LIMIT, CLAMP_LIMIT)
    act = (up + 1.0) * gate * jax.nn.sigmoid(SIGMOID_SLOPE * gate)
    act_ref[...] = act.astype(jnp.bfloat16)


def down_part(where, own_ref, other_ref, down_ref, down_other_ref):
    width = own_ref.shape[1]
    columns = pl.ds(pl.multiple_of(ahead(*where) * width, width), width)
    total = jnp.dot(own_ref[...], down_ref[:, columns], preferred_element_type=jnp.float32)
    total += jnp.dot(
        other_ref[...], down_other_ref[:, columns], preferred_element_type=jnp.float32
    )
    return total.astype(jnp.bfloat16)


def far_kernel(where, own_ref, other_ref, down_ref, down_other_ref, out_ref):
    out_ref[...] = down_part(where, own_ref, other_ref, down_ref, down_other_ref)


def rest_kernel(chips, *refs):
    acts, weights, (other_ref, near_a_ref, near_b_ref, kept_ref) = refs[:4], refs[4:6], refs[6:]
    for part in range(2):
        half = acts[2 * part : 2 * part + 2]
        at = slice(part * half[0].shape[0], (part + 1) * half[0].shape[0])
        other_ref[at, :] = down_part((1, 1, chips), *half, *weights)
        near_ref = near_b_ref if part else near_a_ref
        near_ref[...] = down_part((1, 0, chips), *half, *weights)
        kept_ref[at, :] = down_part((0, 0, chips), *half, *weights)


def sum_kernel(kept_ref, other_ref, near_a_ref, near_b_ref, out_ref):
    half = near_a_ref.shape[0]
    for part, near_ref in enumerate((near_a_ref, near_b_ref)):
        at = slice(part * half, (part + 1) * half)
        total = kept_ref[at, :].astype(jnp.float32) + other_ref[at, :].astype(jnp.float32)
        out_ref[at, :] = (total + near_ref[...].astype(jnp.float32)).astype(jnp.bfloat16)


def combine_kernel(share_ref, rows_ref, mix_ref, squares_ref):
    tokens = mix_ref.shape[0]
    parts = jnp.dot(share_ref[...], rows_ref[...], preferred_element_type=jnp.float32)
    mix = parts[:tokens] + parts[tokens : 2 * tokens] + parts[2 * tokens :]
    mix_ref[...] = mix
    ones = jnp.ones((8, mix.shape[1]), jnp.bfloat16)
    sums = functools.reduce(jnp.add, [dot_t(ones, part) for part in split3(mix * mix)])
    sums = jnp.concatenate([sums, jnp.zeros_like(sums)], axis=1)
    for i in range(squares_ref.shape[0]):
        squares_ref[i] = sums[0:1]


def final_kernel(model_width, mix_ref, squares_ref, gain_ref, out_ref):
    total = squares_ref[0]
    for i in range(1, squares_ref.shape[0]):
        total += squares_ref[i]
    mix = mix_ref[...]
    tokens = mix.shape[0]
    wide = jnp.broadcast_to(total, (tokens, total.shape[1]))
    row = lax.broadcasted_iota(jnp.int32, wide.shape, 0)
    lane = lax.broadcasted_iota(jnp.int32, wide.shape, 1)
    column = jnp.sum(jnp.where(row == lane, wide, 0.0), axis=1, keepdims=True)
    scale = lax.rsqrt(column / model_width + EPSILON)
    out_ref[...] = (mix * scale * gain_ref[...]).astype(jnp.bfloat16)


def call(kernel, outs, *args, limit=8, flops=0, space=VMEM, scratch=()):
    single = not isinstance(outs, (list, tuple))
    if space is HBM:
        args = [pltpu.with_memory_space_constraint(arg, pltpu.HBM) for arg in args]
    return pl.pallas_call(
        kernel,
        out_shape=outs,
        in_specs=[space] * len(args),
        out_specs=VMEM if single else [VMEM] * len(outs),
        scratch_shapes=scratch,
        cost_estimate=pl.CostEstimate(flops=flops, bytes_accessed=0, transcendentals=0),
        compiler_params=pltpu.CompilerParams(vmem_limit_bytes=limit << 20),
    )(*args)


def shape_of(dims, dtype):
    return jax.ShapeDtypeStruct(dims, dtype)


def local(tokens, norm_gain, expert_ids, route_weights, gate_proj, up_proj, down_proj, final_gain):
    tok_rows, width = tokens.shape
    peers = lax.axis_size("tp")
    experts = lax.axis_size("ep")
    chips = peers // CORES
    capacity = min(tok_rows, 2 * tok_rows * expert_ids.shape[1] // experts)
    rows = experts * capacity
    model_width = width * peers

    def onward(value):
        pairs = [
            (y * CORES + c, ((y + 1 - 2 * c) % chips) * CORES + c)
            for y in range(chips)
            for c in range(CORES)
        ]
        return lax.ppermute(value, "tp", pairs)

    def swap(value):
        pairs = [(y * CORES + c, y * CORES + 1 - c) for y in range(chips) for c in range(CORES)]
        return lax.ppermute(value, "tp", pairs)

    narrow = shape_of((rows, width), jnp.bfloat16)
    ids = expert_ids.T
    outbound, gain = call(
        functools.partial(pick_kernel, experts, capacity),
        [narrow, shape_of((1, width), jnp.float32)],
        ids,
        tokens,
        norm_gain[None, :],
        space=HBM,
        scratch=(
            pltpu.VMEM(ids.shape, jnp.int32),
            pltpu.VMEM(tokens.shape, jnp.bfloat16),
            pltpu.SemaphoreType.DMA((3,)),
        ),
    )
    received = lax.all_to_all(
        outbound.reshape(experts, capacity, width), "ep", split_axis=0, concat_axis=0, tiled=True
    ).reshape(rows, width)
    half = rows // 2
    whole, head, rest = [
        shape_of((n, width), jnp.bfloat16) for n in (rows + TAIL, half + TAIL, half)
    ]
    own, own_a, own_b = call(mid_kernel, [whole, head, rest], received, gain)

    first_a = onward(own_a)
    own_other = swap(own)
    first_b = onward(own_b)
    second = onward(own_other)
    third_a = onward(first_a)
    third_b = onward(first_b)
    first_other = (swap(first_a), swap(first_b))
    second_other = swap(second)
    third_other_a = swap(third_a)
    third_other_b = swap(third_b)
    sources = (ids, route_weights.T, final_gain[None, :], up_proj[0])
    share, final_gain, up = call(
        functools.partial(load_kernel, experts, capacity),
        [shape_of((3 * tok_rows, rows), jnp.bfloat16)]
        + [shape_of(source.shape, source.dtype) for source in sources[2:]],
        *sources,
        space=HBM,
        scratch=(
            pltpu.VMEM(ids.shape, jnp.int32),
            pltpu.VMEM(ids.shape, jnp.float32),
            pltpu.SemaphoreType.DMA((len(sources),)),
        ),
    )
    gate, down = gate_proj[0], down_proj[0]
    down_other = swap(down)
    early = [
        ((0, 0, chips), (own,)),
        ((0, 1, chips), (own_other,)),
        ((-1, 0, chips), (first_a, first_b)),
        ((1, 1, chips), first_other),
        ((-1, 1, chips), (second,)),
        ((1, 0, chips), (second_other,)),
    ]
    late = [(-2, 0, chips), (2, 1, chips)]
    wide = shape_of((rows, width), jnp.float32)
    flops = 4 * rows * width * width
    sums = call(
        functools.partial(
            first_kernel, [where for where, _ in early], [len(held) for _, held in early]
        ),
        [wide, wide, shape_of((rows, 128), jnp.float32)],
        *[part for _, held in early for part in held],
        gate,
        up,
        limit=16,
        flops=len(early) * flops,
    )

    def last(part, *held):
        act = call(
            functools.partial(last_kernel, late, [len(held) // 2] * 2, part),
            rest,
            *held,
            gate,
            up,
            *sums,
            limit=16,
            flops=flops,
        )
        return act, swap(act)

    act_a = last(0, third_a, third_other_a)
    act_b = last(1, third_a, third_b, third_other_a, third_other_b)

    def far(acts):
        out = call(
            functools.partial(far_kernel, (2, 0, chips)),
            rest,
            *acts,
            down,
            down_other,
            limit=16,
            flops=flops // 2,
        )
        return onward(out)

    far_a = far(act_a)
    far_b = far(act_b)
    narrow = shape_of((rows, width), jnp.bfloat16)
    near_other, near_a, near_b, kept = call(
        functools.partial(rest_kernel, chips),
        [narrow, rest, rest, narrow],
        *act_a,
        *act_b,
        down,
        down_other,
        limit=16,
        flops=3 * flops,
    )
    near_other = onward(near_other)

    def near(mine, came):
        total = mine.astype(jnp.float32) + came.astype(jnp.float32)
        return onward(total.astype(jnp.bfloat16))

    near_a = near(near_a, far_a)
    near_b = near(near_b, far_b)
    near_other = swap(near_other)
    total = call(sum_kernel, narrow, kept, near_other, near_a, near_b)
    expert_out = total.reshape(experts, capacity, width)
    returned = lax.all_to_all(expert_out, "ep", split_axis=0, concat_axis=0, tiled=True)
    mixture, squares = call(
        combine_kernel,
        [shape_of((tok_rows, width), jnp.float32), shape_of((peers, 1, 128), jnp.float32)],
        share,
        returned.reshape(rows, width),
    )
    squares = lax.all_to_all(squares, "tp", split_axis=0, concat_axis=0, tiled=True)
    return call(
        functools.partial(final_kernel, model_width),
        shape_of((tok_rows, width), jnp.bfloat16),
        mixture,
        squares,
        final_gain,
    )


def solution(mesh):
    placed = (
        P("ep", "tp"),
        P("tp"),
        P("ep", None),
        P("ep", None),
        P("ep", None, "tp"),
        P("ep", None, "tp"),
        P("ep", "tp", None),
        P("tp"),
    )

    return jax.shard_map(
        local, mesh=mesh, in_specs=placed, out_specs=P("ep", "tp"), check_vma=False
    )
```

```python
import functools

import jax
import jax.numpy as jnp
from jax import lax
from jax.experimental import pallas as pl
from jax.experimental.pallas import tpu as pltpu
from jax.sharding import PartitionSpec as P


EPSILON = 1e-05
CLAMP_LIMIT = 7.0
SIGMOID_SLOPE = 1.702
CORES = 2
TAIL = 16
VMEM = pl.BlockSpec(memory_space=pltpu.VMEM)
HBM = pl.BlockSpec(memory_space=pltpu.HBM)


def split3(v):
    hi = v.astype(jnp.bfloat16)
    rest = v - hi.astype(jnp.float32)
    mid = rest.astype(jnp.bfloat16)
    lo = (rest - mid.astype(jnp.float32)).astype(jnp.bfloat16)
    return hi, mid, lo


def dot_t(a, b):
    return lax.dot_general(a, b, (((1,), (1,)), ((), ())), preferred_element_type=jnp.float32)


def dot_0(a, b):
    return lax.dot_general(a, b, (((0,), (0,)), ((), ())), preferred_element_type=jnp.float32)


def slot_matrix(ids, experts, capacity):
    choices, tokens = ids.shape
    expert = lax.broadcasted_iota(jnp.int32, (experts, tokens), 0)
    named = [(ids[k : k + 1, :] == expert).astype(jnp.float32) for k in range(choices)]
    match = functools.reduce(jnp.add, named)
    before = lax.broadcasted_iota(jnp.int32, (tokens, tokens), 0)
    after = lax.broadcasted_iota(jnp.int32, (tokens, tokens), 1)
    earlier = (before < after).astype(jnp.bfloat16)
    place = jnp.dot(match.astype(jnp.bfloat16), earlier, preferred_element_type=jnp.float32)
    place = jnp.where(match > 0.0, place, -1.0)

    def spread(rows):
        wide = jnp.broadcast_to(rows[:, None, :], (experts, capacity, tokens))
        return wide.reshape(experts * capacity, tokens)

    slot = lax.broadcasted_iota(jnp.int32, (experts, capacity, tokens), 1)
    slot = slot.reshape(experts * capacity, tokens).astype(jnp.float32)
    holds = spread(place) == slot
    return holds, named, spread


def pick_kernel(experts, capacity, ids_hbm, tokens_hbm, gain_hbm, rows_ref, gain_ref, ids_ref, tokens_ref, sems):
    copies = [
        pltpu.make_async_copy(ids_hbm, ids_ref, sems.at[0]),
        pltpu.make_async_copy(tokens_hbm, tokens_ref, sems.at[1]),
        pltpu.make_async_copy(gain_hbm, gain_ref, sems.at[2]),
    ]
    for copy in copies:
        copy.start()
    copies[0].wait()
    holds, _, _ = slot_matrix(ids_ref[...], experts, capacity)
    holds = holds.astype(jnp.bfloat16)
    copies[1].wait()
    picked = jnp.dot(holds, tokens_ref[...], preferred_element_type=jnp.float32)
    rows_ref[...] = picked.astype(jnp.bfloat16)
    copies[2].wait()


def load_kernel(experts, capacity, *refs):
    *refs, ids_ref, weights_ref, sems = refs
    count = (len(refs) + 1) // 2
    ids_hbm, weights_hbm, *sources = refs[:count]
    share_ref, *targets = refs[count:]
    pairs = [(ids_hbm, ids_ref), (weights_hbm, weights_ref), *zip(sources, targets)]
    copies = [pltpu.make_async_copy(*pair, sems.at[i]) for i, pair in enumerate(pairs)]
    for copy in copies:
        copy.start()
    copies[0].wait()
    holds, named, spread = slot_matrix(ids_ref[...], experts, capacity)
    copies[1].wait()
    weights = weights_ref[...]
    share = functools.reduce(
        jnp.add, [weights[k : k + 1, :] * named[k] for k in range(len(named))]
    )
    share = jnp.where(holds, spread(share), 0.0).T
    tokens = share.shape[0]
    for i, part in enumerate(split3(share)):
        share_ref[i * tokens : (i + 1) * tokens, :] = part
    for copy in copies[2:]:
        copy.wait()


def mid_kernel(rows_ref, gain_ref, out_ref, out_a_ref, out_b_ref):
    rows, width = rows_ref.shape
    half = rows // 2
    x = rows_ref[...].astype(jnp.float32)
    scaled = (x * gain_ref[...]).astype(jnp.bfloat16)
    out_ref[0:rows, :] = scaled
    out_a_ref[0:half, :] = scaled[:half]
    out_b_ref[...] = scaled[half:]
    hi, mid, _ = split3(x * x)
    ones = jnp.ones((8, width), jnp.bfloat16)
    sums = dot_t(ones, hi) + dot_t(ones, mid)
    row = lax.broadcasted_iota(jnp.int32, (8, width), 0)
    tail = []
    for part in range(rows // width):
        pieces = [v.astype(jnp.float32) for v in split3(sums[:, part * width : (part + 1) * width])]
        tail.append(
            jnp.where(
                row == 0,
                pieces[0],
                jnp.where(row == 1, pieces[1], jnp.where(row == 2, pieces[2], 0.0)),
            )
        )
    tail = jnp.concatenate(tail, axis=0).astype(jnp.bfloat16)
    out_ref[rows : rows + TAIL, :] = tail
    out_a_ref[half : half + TAIL, :] = tail


def ahead(step, other, chips):
    me = lax.axis_index("tp")
    core = me % CORES
    return (me // CORES + step * (1 - 2 * core) + chips) % chips * CORES + (core + other) % CORES


def products(part, pieces, gate_ref, up_ref, gate, up, squares):
    width = gate_ref.shape[1]
    row = lax.broadcasted_iota(jnp.int32, (TAIL, 128), 0)
    ones = jnp.where(row // 8 == part, 1.0, 0.0).astype(jnp.bfloat16)
    for where, refs in pieces:
        from_row = pl.ds(pl.multiple_of(ahead(*where) * width, width), width)
        at = part * width if len(refs) == 1 else 0
        x = refs[part if len(refs) > 1 else 0][at : at + width, :]
        end = refs[0].shape[0]
        gate += jnp.dot(x, gate_ref[from_row, :], preferred_element_type=jnp.float32)
        up += jnp.dot(x, up_ref[from_row, :], preferred_element_type=jnp.float32)
        squares += dot_0(refs[0][end - TAIL : end, :], ones)
    return gate, up, squares


def grouped(places, sizes, refs):
    pieces, at = [], 0
    for where, size in zip(places, sizes):
        pieces.append((where, refs[at : at + size]))
        at += size
    return pieces, refs[at:]


def first_kernel(places, sizes, *refs):
    pieces, (gate_ref, up_ref, *before, gate_out, up_out, squares_out) = grouped(
        places, sizes, refs
    )
    width = gate_ref.shape[1]
    for part in range(gate_out.shape[0] // width):
        at = slice(part * width, (part + 1) * width)
        zero = jnp.zeros((width, width), jnp.float32)
        start = [ref[at, :] for ref in before] or [zero, zero, zero[:, :128]]
        gate, up, squares = products(part, pieces, gate_ref, up_ref, *start)
        gate_out[at, :] = gate
        up_out[at, :] = up
        squares_out[at, :] = squares


def last_kernel(places, sizes, part, *refs):
    pieces, refs = grouped(places, sizes, refs)
    gate_ref, up_ref, gate_in, up_in, squares_in, act_ref = refs
    model_width, width = gate_ref.shape
    at = slice(part * width, (part + 1) * width)
    gate, up, squares = products(
        part, pieces, gate_ref, up_ref, gate_in[at, :], up_in[at, :], squares_in[at, :]
    )
    scale = lax.rsqrt(squares / model_width + EPSILON)
    scale = jnp.concatenate([scale] * (width // 128), axis=1)
    gate = jnp.minimum(gate * scale, CLAMP_LIMIT)
    up = jnp.clip(up * scale, -CLAMP_LIMIT, CLAMP_LIMIT)
    act = (up + 1.0) * gate * jax.nn.sigmoid(SIGMOID_SLOPE * gate)
    act_ref[...] = act.astype(jnp.bfloat16)


def down_part(where, own_ref, other_ref, down_ref, down_other_ref):
    width = own_ref.shape[1]
    columns = pl.ds(pl.multiple_of(ahead(*where) * width, width), width)
    total = jnp.dot(own_ref[...], down_ref[:, columns], preferred_element_type=jnp.float32)
    total += jnp.dot(
        other_ref[...], down_other_ref[:, columns], preferred_element_type=jnp.float32
    )
    return total.astype(jnp.bfloat16)


def far_kernel(where, own_ref, other_ref, down_ref, down_other_ref, out_ref):
    out_ref[...] = down_part(where, own_ref, other_ref, down_ref, down_other_ref)


def rest_kernel(chips, *refs):
    acts, weights, (other_ref, near_a_ref, near_b_ref, kept_ref) = refs[:4], refs[4:6], refs[6:]
    for part in range(2):
        half = acts[2 * part : 2 * part + 2]
        at = slice(part * half[0].shape[0], (part + 1) * half[0].shape[0])
        other_ref[at, :] = down_part((1, 1, chips), *half, *weights)
        near_ref = near_b_ref if part else near_a_ref
        near_ref[...] = down_part((1, 0, chips), *half, *weights)
        kept_ref[at, :] = down_part((0, 0, chips), *half, *weights)


def sum_kernel(kept_ref, other_ref, near_a_ref, near_b_ref, out_ref):
    half = near_a_ref.shape[0]
    for part, near_ref in enumerate((near_a_ref, near_b_ref)):
        at = slice(part * half, (part + 1) * half)
        total = kept_ref[at, :].astype(jnp.float32) + other_ref[at, :].astype(jnp.float32)
        out_ref[at, :] = (total + near_ref[...].astype(jnp.float32)).astype(jnp.bfloat16)


def combine_kernel(share_ref, rows_ref, mix_ref, squares_ref):
    tokens = mix_ref.shape[0]
    parts = jnp.dot(share_ref[...], rows_ref[...], preferred_element_type=jnp.float32)
    mix = parts[:tokens] + parts[tokens : 2 * tokens] + parts[2 * tokens :]
    mix_ref[...] = mix
    ones = jnp.ones((8, mix.shape[1]), jnp.bfloat16)
    sums = functools.reduce(jnp.add, [dot_t(ones, part) for part in split3(mix * mix)])
    sums = jnp.concatenate([sums, jnp.zeros_like(sums)], axis=1)
    for i in range(squares_ref.shape[0]):
        squares_ref[i] = sums[0:1]


def final_kernel(model_width, mix_ref, squares_ref, gain_ref, out_ref):
    total = squares_ref[0]
    for i in range(1, squares_ref.shape[0]):
        total += squares_ref[i]
    mix = mix_ref[...]
    tokens = mix.shape[0]
    wide = jnp.broadcast_to(total, (tokens, total.shape[1]))
    row = lax.broadcasted_iota(jnp.int32, wide.shape, 0)
    lane = lax.broadcasted_iota(jnp.int32, wide.shape, 1)
    column = jnp.sum(jnp.where(row == lane, wide, 0.0), axis=1, keepdims=True)
    scale = lax.rsqrt(column / model_width + EPSILON)
    out_ref[...] = (mix * scale * gain_ref[...]).astype(jnp.bfloat16)


def call(kernel, outs, *args, limit=8, flops=0, space=VMEM, scratch=()):
    single = not isinstance(outs, (list, tuple))
    if space is HBM:
        args = [pltpu.with_memory_space_constraint(arg, pltpu.HBM) for arg in args]
    return pl.pallas_call(
        kernel,
        out_shape=outs,
        in_specs=[space] * len(args),
        out_specs=VMEM if single else [VMEM] * len(outs),
        scratch_shapes=scratch,
        cost_estimate=pl.CostEstimate(flops=flops, bytes_accessed=0, transcendentals=0),
        compiler_params=pltpu.CompilerParams(vmem_limit_bytes=limit << 20),
    )(*args)


def shape_of(dims, dtype):
    return jax.ShapeDtypeStruct(dims, dtype)


def local(tokens, norm_gain, expert_ids, route_weights, gate_proj, up_proj, down_proj, final_gain):
    tok_rows, width = tokens.shape
    peers = lax.axis_size("tp")
    experts = lax.axis_size("ep")
    chips = peers // CORES
    capacity = min(tok_rows, 2 * tok_rows * expert_ids.shape[1] // experts)
    rows = experts * capacity
    model_width = width * peers

    def onward(value):
        pairs = [
            (y * CORES + c, ((y + 1 - 2 * c) % chips) * CORES + c)
            for y in range(chips)
            for c in range(CORES)
        ]
        return lax.ppermute(value, "tp", pairs)

    def swap(value):
        pairs = [(y * CORES + c, y * CORES + 1 - c) for y in range(chips) for c in range(CORES)]
        return lax.ppermute(value, "tp", pairs)

    narrow = shape_of((rows, width), jnp.bfloat16)
    ids = expert_ids.T
    outbound, gain = call(
        functools.partial(pick_kernel, experts, capacity),
        [narrow, shape_of((1, width), jnp.float32)],
        ids,
        tokens,
        norm_gain[None, :],
        space=HBM,
        scratch=(
            pltpu.VMEM(ids.shape, jnp.int32),
            pltpu.VMEM(tokens.shape, jnp.bfloat16),
            pltpu.SemaphoreType.DMA((3,)),
        ),
    )
    received = lax.all_to_all(
        outbound.reshape(experts, capacity, width), "ep", split_axis=0, concat_axis=0, tiled=True
    ).reshape(rows, width)
    half = rows // 2
    whole, head, rest = [
        shape_of((n, width), jnp.bfloat16) for n in (rows + TAIL, half + TAIL, half)
    ]
    own, own_a, own_b = call(mid_kernel, [whole, head, rest], received, gain)

    first_a = onward(own_a)
    own_other = swap(own)
    first_b = onward(own_b)
    second = onward(own_other)
    third_a = onward(first_a)
    third_b = onward(first_b)
    first_other = (swap(first_a), swap(first_b))
    second_other = swap(second)
    third_other_a = swap(third_a)
    third_other_b = swap(third_b)
    sources = (ids, route_weights.T, final_gain[None, :], up_proj[0])
    share, final_gain, up = call(
        functools.partial(load_kernel, experts, capacity),
        [shape_of((3 * tok_rows, rows), jnp.bfloat16)]
        + [shape_of(source.shape, source.dtype) for source in sources[2:]],
        *sources,
        space=HBM,
        scratch=(
            pltpu.VMEM(ids.shape, jnp.int32),
            pltpu.VMEM(ids.shape, jnp.float32),
            pltpu.SemaphoreType.DMA((len(sources),)),
        ),
    )
    gate, down = gate_proj[0], down_proj[0]
    down_other = swap(down)
    early = [
        ((0, 0, chips), (own,)),
        ((0, 1, chips), (own_other,)),
        ((-1, 0, chips), (first_a, first_b)),
        ((1, 1, chips), first_other),
        ((-1, 1, chips), (second,)),
        ((1, 0, chips), (second_other,)),
    ]
    late = [(-2, 0, chips), (2, 1, chips)]
    wide = shape_of((rows, width), jnp.float32)
    flops = 4 * rows * width * width

    def sums_of(pieces, *before):
        return call(
            functools.partial(
                first_kernel, [where for where, _ in pieces], [len(held) for _, held in pieces]
            ),
            [wide, wide, shape_of((rows, 128), jnp.float32)],
            *[part for _, held in pieces for part in held],
            gate,
            up,
            *before,
            limit=16,
            flops=len(pieces) * flops,
        )

    sums = sums_of(early[4:], *sums_of(early[:4]))

    def last(part, *held):
        act = call(
            functools.partial(last_kernel, late, [len(held) // 2] * 2, part),
            rest,
            *held,
            gate,
            up,
            *sums,
            limit=16,
            flops=flops,
        )
        return act, swap(act)

    act_a = last(0, third_a, third_other_a)
    act_b = last(1, third_a, third_b, third_other_a, third_other_b)

    def far(acts):
        out = call(
            functools.partial(far_kernel, (2, 0, chips)),
            rest,
            *acts,
            down,
            down_other,
            limit=16,
            flops=flops // 2,
        )
        return onward(out)

    far_a = far(act_a)
    far_b = far(act_b)
    narrow = shape_of((rows, width), jnp.bfloat16)
    near_other, near_a, near_b, kept = call(
        functools.partial(rest_kernel, chips),
        [narrow, rest, rest, narrow],
        *act_a,
        *act_b,
        down,
        down_other,
        limit=16,
        flops=3 * flops,
    )
    near_other = onward(near_other)

    def near(mine, came):
        total = mine.astype(jnp.float32) + came.astype(jnp.float32)
        return onward(total.astype(jnp.bfloat16))

    near_a = near(near_a, far_a)
    near_b = near(near_b, far_b)
    near_other = swap(near_other)
    total = call(sum_kernel, narrow, kept, near_other, near_a, near_b)
    expert_out = total.reshape(experts, capacity, width)
    returned = lax.all_to_all(expert_out, "ep", split_axis=0, concat_axis=0, tiled=True)
    mixture, squares = call(
        combine_kernel,
        [shape_of((tok_rows, width), jnp.float32), shape_of((peers, 1, 128), jnp.float32)],
        share,
        returned.reshape(rows, width),
    )
    squares = lax.all_to_all(squares, "tp", split_axis=0, concat_axis=0, tiled=True)
    return call(
        functools.partial(final_kernel, model_width),
        shape_of((tok_rows, width), jnp.bfloat16),
        mixture,
        squares,
        final_gain,
    )


def solution(mesh):
    placed = (
        P("ep", "tp"),
        P("tp"),
        P("ep", None),
        P("ep", None),
        P("ep", None, "tp"),
        P("ep", None, "tp"),
        P("ep", "tp", None),
        P("tp"),
    )

    return jax.shard_map(
        local, mesh=mesh, in_specs=placed, out_specs=P("ep", "tp"), check_vma=False
    )
```

```python
import functools

import jax
import jax.numpy as jnp
from jax import lax
from jax.experimental import pallas as pl
from jax.experimental.pallas import tpu as pltpu
from jax.sharding import PartitionSpec as P


EPSILON = 1e-05
CLAMP_LIMIT = 7.0
SIGMOID_SLOPE = 1.702
CORES = 2
TAIL = 16
VMEM = pl.BlockSpec(memory_space=pltpu.VMEM)
HBM = pl.BlockSpec(memory_space=pltpu.HBM)


def split3(v):
    hi = v.astype(jnp.bfloat16)
    rest = v - hi.astype(jnp.float32)
    mid = rest.astype(jnp.bfloat16)
    lo = (rest - mid.astype(jnp.float32)).astype(jnp.bfloat16)
    return hi, mid, lo


def dot_t(a, b):
    return lax.dot_general(a, b, (((1,), (1,)), ((), ())), preferred_element_type=jnp.float32)


def dot_0(a, b):
    return lax.dot_general(a, b, (((0,), (0,)), ((), ())), preferred_element_type=jnp.float32)


def slot_matrix(ids, experts, capacity):
    choices, tokens = ids.shape
    expert = lax.broadcasted_iota(jnp.int32, (experts, tokens), 0)
    named = [(ids[k : k + 1, :] == expert).astype(jnp.float32) for k in range(choices)]
    match = functools.reduce(jnp.add, named)
    before = lax.broadcasted_iota(jnp.int32, (tokens, tokens), 0)
    after = lax.broadcasted_iota(jnp.int32, (tokens, tokens), 1)
    earlier = (before < after).astype(jnp.bfloat16)
    place = jnp.dot(match.astype(jnp.bfloat16), earlier, preferred_element_type=jnp.float32)
    place = jnp.where(match > 0.0, place, -1.0)

    def spread(rows):
        wide = jnp.broadcast_to(rows[:, None, :], (experts, capacity, tokens))
        return wide.reshape(experts * capacity, tokens)

    slot = lax.broadcasted_iota(jnp.int32, (experts, capacity, tokens), 1)
    slot = slot.reshape(experts * capacity, tokens).astype(jnp.float32)
    holds = spread(place) == slot
    return holds, named, spread


def pick_kernel(experts, capacity, ids_hbm, tokens_hbm, gain_hbm, rows_ref, gain_ref, ids_ref, tokens_ref, sems):
    copies = [
        pltpu.make_async_copy(ids_hbm, ids_ref, sems.at[0]),
        pltpu.make_async_copy(tokens_hbm, tokens_ref, sems.at[1]),
        pltpu.make_async_copy(gain_hbm, gain_ref, sems.at[2]),
    ]
    for copy in copies:
        copy.start()
    copies[0].wait()
    holds, _, _ = slot_matrix(ids_ref[...], experts, capacity)
    holds = holds.astype(jnp.bfloat16)
    copies[1].wait()
    picked = jnp.dot(holds, tokens_ref[...], preferred_element_type=jnp.float32)
    rows_ref[...] = picked.astype(jnp.bfloat16)
    copies[2].wait()


def load_kernel(experts, capacity, *refs):
    *refs, ids_ref, weights_ref, sems = refs
    count = (len(refs) + 1) // 2
    ids_hbm, weights_hbm, *sources = refs[:count]
    share_ref, *targets = refs[count:]
    pairs = [(ids_hbm, ids_ref), (weights_hbm, weights_ref), *zip(sources, targets)]
    copies = [pltpu.make_async_copy(*pair, sems.at[i]) for i, pair in enumerate(pairs)]
    for copy in copies:
        copy.start()
    copies[0].wait()
    holds, named, spread = slot_matrix(ids_ref[...], experts, capacity)
    copies[1].wait()
    weights = weights_ref[...]
    share = functools.reduce(
        jnp.add, [weights[k : k + 1, :] * named[k] for k in range(len(named))]
    )
    share = jnp.where(holds, spread(share), 0.0).T
    tokens = share.shape[0]
    for i, part in enumerate(split3(share)):
        share_ref[i * tokens : (i + 1) * tokens, :] = part
    for copy in copies[2:]:
        copy.wait()


def mid_kernel(rows_ref, gain_ref, out_ref, out_a_ref, out_b_ref):
    rows, width = rows_ref.shape
    half = rows // 2
    x = rows_ref[...].astype(jnp.float32)
    scaled = (x * gain_ref[...]).astype(jnp.bfloat16)
    out_ref[0:rows, :] = scaled
    out_a_ref[0:half, :] = scaled[:half]
    out_b_ref[...] = scaled[half:]
    hi, mid, _ = split3(x * x)
    ones = jnp.ones((8, width), jnp.bfloat16)
    sums = dot_t(ones, hi) + dot_t(ones, mid)
    row = lax.broadcasted_iota(jnp.int32, (8, width), 0)
    tail = []
    for part in range(rows // width):
        pieces = [v.astype(jnp.float32) for v in split3(sums[:, part * width : (part + 1) * width])]
        tail.append(
            jnp.where(
                row == 0,
                pieces[0],
                jnp.where(row == 1, pieces[1], jnp.where(row == 2, pieces[2], 0.0)),
            )
        )
    tail = jnp.concatenate(tail, axis=0).astype(jnp.bfloat16)
    out_ref[rows : rows + TAIL, :] = tail
    out_a_ref[half : half + TAIL, :] = tail


def ahead(step, other, chips):
    me = lax.axis_index("tp")
    core = me % CORES
    return (me // CORES + step * (1 - 2 * core) + chips) % chips * CORES + (core + other) % CORES


def products(part, pieces, gate_ref, up_ref, gate, up, squares):
    width = gate_ref.shape[1]
    row = lax.broadcasted_iota(jnp.int32, (TAIL, 128), 0)
    ones = jnp.where(row // 8 == part, 1.0, 0.0).astype(jnp.bfloat16)
    for where, refs in pieces:
        from_row = pl.ds(pl.multiple_of(ahead(*where) * width, width), width)
        at = part * width if len(refs) == 1 else 0
        x = refs[part if len(refs) > 1 else 0][at : at + width, :]
        end = refs[0].shape[0]
        gate += jnp.dot(x, gate_ref[from_row, :], preferred_element_type=jnp.float32)
        up += jnp.dot(x, up_ref[from_row, :], preferred_element_type=jnp.float32)
        squares += dot_0(refs[0][end - TAIL : end, :], ones)
    return gate, up, squares


def grouped(places, sizes, refs):
    pieces, at = [], 0
    for where, size in zip(places, sizes):
        pieces.append((where, refs[at : at + size]))
        at += size
    return pieces, refs[at:]


def first_kernel(places, sizes, *refs):
    pieces, (gate_ref, up_ref, *before, gate_out, up_out, squares_out) = grouped(
        places, sizes, refs
    )
    width = gate_ref.shape[1]
    for part in range(gate_out.shape[0] // width):
        at = slice(part * width, (part + 1) * width)
        zero = jnp.zeros((width, width), jnp.float32)
        start = [ref[at, :] for ref in before] or [zero, zero, zero[:, :128]]
        gate, up, squares = products(part, pieces, gate_ref, up_ref, *start)
        gate_out[at, :] = gate
        up_out[at, :] = up
        squares_out[at, :] = squares


def last_kernel(places, sizes, part, *refs):
    pieces, refs = grouped(places, sizes, refs)
    gate_ref, up_ref, gate_in, up_in, squares_in, act_ref = refs
    model_width, width = gate_ref.shape
    at = slice(part * width, (part + 1) * width)
    gate, up, squares = products(
        part, pieces, gate_ref, up_ref, gate_in[at, :], up_in[at, :], squares_in[at, :]
    )
    scale = lax.rsqrt(squares / model_width + EPSILON)
    scale = jnp.concatenate([scale] * (width // 128), axis=1)
    gate = jnp.minimum(gate * scale, CLAMP_LIMIT)
    up = jnp.clip(up * scale, -CLAMP_LIMIT, CLAMP_LIMIT)
    act = (up + 1.0) * gate * jax.nn.sigmoid(SIGMOID_SLOPE * gate)
    act_ref[...] = act.astype(jnp.bfloat16)


def down_part(where, own_ref, other_ref, down_ref, down_other_ref):
    width = own_ref.shape[1]
    columns = pl.ds(pl.multiple_of(ahead(*where) * width, width), width)
    total = jnp.dot(own_ref[...], down_ref[:, columns], preferred_element_type=jnp.float32)
    total += jnp.dot(
        other_ref[...], down_other_ref[:, columns], preferred_element_type=jnp.float32
    )
    return total.astype(jnp.bfloat16)


def far_kernel(where, own_ref, other_ref, down_ref, down_other_ref, out_ref):
    out_ref[...] = down_part(where, own_ref, other_ref, down_ref, down_other_ref)


def rest_kernel(chips, *refs):
    acts, weights, (other_ref, near_a_ref, near_b_ref, kept_ref) = refs[:4], refs[4:6], refs[6:]
    for part in range(2):
        half = acts[2 * part : 2 * part + 2]
        at = slice(part * half[0].shape[0], (part + 1) * half[0].shape[0])
        other_ref[at, :] = down_part((1, 1, chips), *half, *weights)
        near_ref = near_b_ref if part else near_a_ref
        near_ref[...] = down_part((1, 0, chips), *half, *weights)
        kept_ref[at, :] = down_part((0, 0, chips), *half, *weights)


def sum_kernel(kept_ref, other_ref, near_a_ref, near_b_ref, out_ref):
    half = near_a_ref.shape[0]
    for part, near_ref in enumerate((near_a_ref, near_b_ref)):
        at = slice(part * half, (part + 1) * half)
        total = kept_ref[at, :].astype(jnp.float32) + other_ref[at, :].astype(jnp.float32)
        out_ref[at, :] = (total + near_ref[...].astype(jnp.float32)).astype(jnp.bfloat16)


def combine_kernel(share_ref, rows_ref, mix_ref, squares_ref):
    tokens = mix_ref.shape[0]
    parts = jnp.dot(share_ref[...], rows_ref[...], preferred_element_type=jnp.float32)
    mix = parts[:tokens] + parts[tokens : 2 * tokens] + parts[2 * tokens :]
    mix_ref[...] = mix
    ones = jnp.ones((8, mix.shape[1]), jnp.bfloat16)
    sums = functools.reduce(jnp.add, [dot_t(ones, part) for part in split3(mix * mix)])
    sums = jnp.concatenate([sums, jnp.zeros_like(sums)], axis=1)
    squares_ref[...] = sums


def final_kernel(model_width, mix_ref, squares_ref, other_ref, gain_ref, out_ref):
    total = squares_ref[0:1, :] + other_ref[0:1, :]
    mix = mix_ref[...]
    tokens = mix.shape[0]
    wide = jnp.broadcast_to(total, (tokens, total.shape[1]))
    row = lax.broadcasted_iota(jnp.int32, wide.shape, 0)
    lane = lax.broadcasted_iota(jnp.int32, wide.shape, 1)
    column = jnp.sum(jnp.where(row == lane, wide, 0.0), axis=1, keepdims=True)
    scale = lax.rsqrt(column / model_width + EPSILON)
    out_ref[...] = (mix * scale * gain_ref[...]).astype(jnp.bfloat16)


def call(kernel, outs, *args, limit=8, flops=0, space=VMEM, scratch=()):
    single = not isinstance(outs, (list, tuple))
    if space is HBM:
        args = [pltpu.with_memory_space_constraint(arg, pltpu.HBM) for arg in args]
    return pl.pallas_call(
        kernel,
        out_shape=outs,
        in_specs=[space] * len(args),
        out_specs=VMEM if single else [VMEM] * len(outs),
        scratch_shapes=scratch,
        cost_estimate=pl.CostEstimate(flops=flops, bytes_accessed=0, transcendentals=0),
        compiler_params=pltpu.CompilerParams(vmem_limit_bytes=limit << 20),
    )(*args)


def shape_of(dims, dtype):
    return jax.ShapeDtypeStruct(dims, dtype)


def local(tokens, norm_gain, expert_ids, route_weights, gate_proj, up_proj, down_proj, final_gain):
    tok_rows, width = tokens.shape
    peers = lax.axis_size("tp")
    experts = lax.axis_size("ep")
    chips = peers // CORES
    capacity = min(tok_rows, 2 * tok_rows * expert_ids.shape[1] // experts)
    rows = experts * capacity
    model_width = width * peers

    def onward(value):
        pairs = [
            (y * CORES + c, ((y + 1 - 2 * c) % chips) * CORES + c)
            for y in range(chips)
            for c in range(CORES)
        ]
        return lax.ppermute(value, "tp", pairs)

    def along(value, step):
        pairs = [
            (y * CORES + c, ((y + step) % chips) * CORES + c)
            for y in range(chips)
            for c in range(CORES)
        ]
        return lax.ppermute(value, "tp", pairs)

    def swap(value):
        pairs = [(y * CORES + c, y * CORES + 1 - c) for y in range(chips) for c in range(CORES)]
        return lax.ppermute(value, "tp", pairs)

    narrow = shape_of((rows, width), jnp.bfloat16)
    ids = expert_ids.T
    outbound, gain = call(
        functools.partial(pick_kernel, experts, capacity),
        [narrow, shape_of((1, width), jnp.float32)],
        ids,
        tokens,
        norm_gain[None, :],
        space=HBM,
        scratch=(
            pltpu.VMEM(ids.shape, jnp.int32),
            pltpu.VMEM(tokens.shape, jnp.bfloat16),
            pltpu.SemaphoreType.DMA((3,)),
        ),
    )
    received = lax.all_to_all(
        outbound.reshape(experts, capacity, width), "ep", split_axis=0, concat_axis=0, tiled=True
    ).reshape(rows, width)
    half = rows // 2
    whole, head, rest = [
        shape_of((n, width), jnp.bfloat16) for n in (rows + TAIL, half + TAIL, half)
    ]
    own, own_a, own_b = call(mid_kernel, [whole, head, rest], received, gain)

    first_a = onward(own_a)
    own_other = swap(own)
    first_b = onward(own_b)
    second = onward(own_other)
    third_a = onward(first_a)
    third_b = onward(first_b)
    first_other = (swap(first_a), swap(first_b))
    second_other = swap(second)
    third_other_a = swap(third_a)
    third_other_b = swap(third_b)
    sources = (ids, route_weights.T, final_gain[None, :], up_proj[0])
    share, final_gain, up = call(
        functools.partial(load_kernel, experts, capacity),
        [shape_of((3 * tok_rows, rows), jnp.bfloat16)]
        + [shape_of(source.shape, source.dtype) for source in sources[2:]],
        *sources,
        space=HBM,
        scratch=(
            pltpu.VMEM(ids.shape, jnp.int32),
            pltpu.VMEM(ids.shape, jnp.float32),
            pltpu.SemaphoreType.DMA((len(sources),)),
        ),
    )
    gate, down = gate_proj[0], down_proj[0]
    down_other = swap(down)
    early = [
        ((0, 0, chips), (own,)),
        ((0, 1, chips), (own_other,)),
        ((-1, 0, chips), (first_a, first_b)),
        ((1, 1, chips), first_other),
        ((-1, 1, chips), (second,)),
        ((1, 0, chips), (second_other,)),
    ]
    late = [(-2, 0, chips), (2, 1, chips)]
    wide = shape_of((rows, width), jnp.float32)
    flops = 4 * rows * width * width

    def sums_of(pieces, *before):
        return call(
            functools.partial(
                first_kernel, [where for where, _ in pieces], [len(held) for _, held in pieces]
            ),
            [wide, wide, shape_of((rows, 128), jnp.float32)],
            *[part for _, held in pieces for part in held],
            gate,
            up,
            *before,
            limit=16,
            flops=len(pieces) * flops,
        )

    sums = sums_of(early[4:], *sums_of(early[:4]))

    def last(part, *held):
        act = call(
            functools.partial(last_kernel, late, [len(held) // 2] * 2, part),
            rest,
            *held,
            gate,
            up,
            *sums,
            limit=16,
            flops=flops,
        )
        return act, swap(act)

    act_a = last(0, third_a, third_other_a)
    act_b = last(1, third_a, third_b, third_other_a, third_other_b)

    def far(acts):
        out = call(
            functools.partial(far_kernel, (2, 0, chips)),
            rest,
            *acts,
            down,
            down_other,
            limit=16,
            flops=flops // 2,
        )
        return onward(out)

    far_a = far(act_a)
    far_b = far(act_b)
    narrow = shape_of((rows, width), jnp.bfloat16)
    near_other, near_a, near_b, kept = call(
        functools.partial(rest_kernel, chips),
        [narrow, rest, rest, narrow],
        *act_a,
        *act_b,
        down,
        down_other,
        limit=16,
        flops=3 * flops,
    )
    near_other = onward(near_other)

    def near(mine, came):
        total = mine.astype(jnp.float32) + came.astype(jnp.float32)
        return onward(total.astype(jnp.bfloat16))

    near_a = near(near_a, far_a)
    near_b = near(near_b, far_b)
    near_other = swap(near_other)
    total = call(sum_kernel, narrow, kept, near_other, near_a, near_b)
    expert_out = total.reshape(experts, capacity, width)
    returned = lax.all_to_all(expert_out, "ep", split_axis=0, concat_axis=0, tiled=True)
    mixture, squares = call(
        combine_kernel,
        [shape_of((tok_rows, width), jnp.float32), shape_of((8, 128), jnp.float32)],
        share,
        returned.reshape(rows, width),
    )
    around = [along(squares, step) for step in (2, 1, chips - 1)]
    squares = functools.reduce(jnp.add, around, squares)
    return call(
        functools.partial(final_kernel, model_width),
        shape_of((tok_rows, width), jnp.bfloat16),
        mixture,
        squares,
        swap(squares),
        final_gain,
    )


def solution(mesh):
    placed = (
        P("ep", "tp"),
        P("tp"),
        P("ep", None),
        P("ep", None),
        P("ep", None, "tp"),
        P("ep", None, "tp"),
        P("ep", "tp", None),
        P("tp"),
    )

    return jax.shard_map(
        local, mesh=mesh, in_specs=placed, out_specs=P("ep", "tp"), check_vma=False
    )
```

```python
import functools

import jax
import jax.numpy as jnp
from jax import lax
from jax.experimental import pallas as pl
from jax.experimental.pallas import tpu as pltpu
from jax.sharding import PartitionSpec as P


EPSILON = 1e-05
CLAMP_LIMIT = 7.0
SIGMOID_SLOPE = 1.702
CORES = 2
TAIL = 16
VMEM = pl.BlockSpec(memory_space=pltpu.VMEM)
HBM = pl.BlockSpec(memory_space=pltpu.HBM)


def split3(v):
    hi = v.astype(jnp.bfloat16)
    rest = v - hi.astype(jnp.float32)
    mid = rest.astype(jnp.bfloat16)
    lo = (rest - mid.astype(jnp.float32)).astype(jnp.bfloat16)
    return hi, mid, lo


def dot_t(a, b):
    return lax.dot_general(a, b, (((1,), (1,)), ((), ())), preferred_element_type=jnp.float32)


def dot_0(a, b):
    return lax.dot_general(a, b, (((0,), (0,)), ((), ())), preferred_element_type=jnp.float32)


def slot_matrix(ids, experts, capacity):
    choices, tokens = ids.shape
    expert = lax.broadcasted_iota(jnp.int32, (experts, tokens), 0)
    named = [(ids[k : k + 1, :] == expert).astype(jnp.float32) for k in range(choices)]
    match = functools.reduce(jnp.add, named)
    before = lax.broadcasted_iota(jnp.int32, (tokens, tokens), 0)
    after = lax.broadcasted_iota(jnp.int32, (tokens, tokens), 1)
    earlier = (before < after).astype(jnp.bfloat16)
    place = jnp.dot(match.astype(jnp.bfloat16), earlier, preferred_element_type=jnp.float32)
    place = jnp.where(match > 0.0, place, -1.0)

    def spread(rows):
        wide = jnp.broadcast_to(rows[:, None, :], (experts, capacity, tokens))
        return wide.reshape(experts * capacity, tokens)

    slot = lax.broadcasted_iota(jnp.int32, (experts, capacity, tokens), 1)
    slot = slot.reshape(experts * capacity, tokens).astype(jnp.float32)
    holds = spread(place) == slot
    return holds, named, spread


def pick_kernel(experts, capacity, ids_hbm, tokens_hbm, gain_hbm, rows_ref, gain_ref, ids_ref, tokens_ref, sems):
    copies = [
        pltpu.make_async_copy(ids_hbm, ids_ref, sems.at[0]),
        pltpu.make_async_copy(tokens_hbm, tokens_ref, sems.at[1]),
        pltpu.make_async_copy(gain_hbm, gain_ref, sems.at[2]),
    ]
    for copy in copies:
        copy.start()
    copies[0].wait()
    holds, _, _ = slot_matrix(ids_ref[...], experts, capacity)
    holds = holds.astype(jnp.bfloat16)
    copies[1].wait()
    picked = jnp.dot(holds, tokens_ref[...], preferred_element_type=jnp.float32)
    rows_ref[...] = picked.astype(jnp.bfloat16)
    copies[2].wait()


def load_kernel(experts, capacity, *refs):
    *refs, ids_ref, weights_ref, sems = refs
    count = (len(refs) + 1) // 2
    ids_hbm, weights_hbm, *sources = refs[:count]
    share_ref, *targets = refs[count:]
    pairs = [(ids_hbm, ids_ref), (weights_hbm, weights_ref), *zip(sources, targets)]
    copies = [pltpu.make_async_copy(*pair, sems.at[i]) for i, pair in enumerate(pairs)]
    for copy in copies:
        copy.start()
    copies[0].wait()
    holds, named, spread = slot_matrix(ids_ref[...], experts, capacity)
    copies[1].wait()
    weights = weights_ref[...]
    share = functools.reduce(
        jnp.add, [weights[k : k + 1, :] * named[k] for k in range(len(named))]
    )
    share = jnp.where(holds, spread(share), 0.0).T
    tokens = share.shape[0]
    for i, part in enumerate(split3(share)):
        share_ref[i * tokens : (i + 1) * tokens, :] = part
    for copy in copies[2:]:
        copy.wait()


def mid_kernel(rows_ref, gain_ref, out_ref, out_a_ref, out_b_ref):
    rows, width = rows_ref.shape
    half = rows // 2
    x = rows_ref[...].astype(jnp.float32)
    scaled = (x * gain_ref[...]).astype(jnp.bfloat16)
    out_ref[0:rows, :] = scaled
    out_a_ref[0:half, :] = scaled[:half]
    out_b_ref[...] = scaled[half:]
    hi, mid, _ = split3(x * x)
    ones = jnp.ones((8, width), jnp.bfloat16)
    sums = dot_t(ones, hi) + dot_t(ones, mid)
    row = lax.broadcasted_iota(jnp.int32, (8, width), 0)
    tail = []
    for part in range(rows // width):
        pieces = [v.astype(jnp.float32) for v in split3(sums[:, part * width : (part + 1) * width])]
        tail.append(
            jnp.where(
                row == 0,
                pieces[0],
                jnp.where(row == 1, pieces[1], jnp.where(row == 2, pieces[2], 0.0)),
            )
        )
    tail = jnp.concatenate(tail, axis=0).astype(jnp.bfloat16)
    out_ref[rows : rows + TAIL, :] = tail
    out_a_ref[half : half + TAIL, :] = tail


def ahead(step, other, chips):
    me = lax.axis_index("tp")
    core = me % CORES
    return (me // CORES + step * (1 - 2 * core) + chips) % chips * CORES + (core + other) % CORES


def products(part, pieces, gate_ref, up_ref, gate, up, squares):
    width = gate_ref.shape[1]
    row = lax.broadcasted_iota(jnp.int32, (TAIL, 128), 0)
    ones = jnp.where(row // 8 == part, 1.0, 0.0).astype(jnp.bfloat16)
    for where, refs in pieces:
        from_row = pl.ds(pl.multiple_of(ahead(*where) * width, width), width)
        at = part * width if len(refs) == 1 else 0
        x = refs[part if len(refs) > 1 else 0][at : at + width, :]
        end = refs[0].shape[0]
        gate += jnp.dot(x, gate_ref[from_row, :], preferred_element_type=jnp.float32)
        up += jnp.dot(x, up_ref[from_row, :], preferred_element_type=jnp.float32)
        squares += dot_0(refs[0][end - TAIL : end, :], ones)
    return gate, up, squares


def grouped(places, sizes, refs):
    pieces, at = [], 0
    for where, size in zip(places, sizes):
        pieces.append((where, refs[at : at + size]))
        at += size
    return pieces, refs[at:]


def first_kernel(places, sizes, *refs):
    pieces, (gate_ref, up_ref, *before, gate_out, up_out, squares_out) = grouped(
        places, sizes, refs
    )
    width = gate_ref.shape[1]
    for part in range(gate_out.shape[0] // width):
        at = slice(part * width, (part + 1) * width)
        zero = jnp.zeros((width, width), jnp.float32)
        start = [ref[at, :] for ref in before] or [zero, zero, zero[:, :128]]
        gate, up, squares = products(part, pieces, gate_ref, up_ref, *start)
        gate_out[at, :] = gate
        up_out[at, :] = up
        squares_out[at, :] = squares


def last_kernel(places, sizes, part, *refs):
    pieces, refs = grouped(places, sizes, refs)
    gate_ref, up_ref, gate_in, up_in, squares_in, act_ref = refs
    model_width, width = gate_ref.shape
    at = slice(part * width, (part + 1) * width)
    gate, up, squares = products(
        part, pieces, gate_ref, up_ref, gate_in[at, :], up_in[at, :], squares_in[at, :]
    )
    scale = lax.rsqrt(squares / model_width + EPSILON)
    scale = jnp.concatenate([scale] * (width // 128), axis=1)
    gate = jnp.minimum(gate * scale, CLAMP_LIMIT)
    up = jnp.clip(up * scale, -CLAMP_LIMIT, CLAMP_LIMIT)
    act = (up + 1.0) * gate * jax.nn.sigmoid(SIGMOID_SLOPE * gate)
    act_ref[...] = act.astype(jnp.bfloat16)


def down_part(where, own_ref, other_ref, down_ref, down_other_ref):
    width = own_ref.shape[1]
    columns = pl.ds(pl.multiple_of(ahead(*where) * width, width), width)
    total = jnp.dot(own_ref[...], down_ref[:, columns], preferred_element_type=jnp.float32)
    total += jnp.dot(
        other_ref[...], down_other_ref[:, columns], preferred_element_type=jnp.float32
    )
    return total.astype(jnp.bfloat16)


def far_kernel(where, own_ref, other_ref, down_ref, down_other_ref, out_ref):
    out_ref[...] = down_part(where, own_ref, other_ref, down_ref, down_other_ref)


def rest_kernel(chips, *refs):
    acts, weights, (other_ref, near_a_ref, near_b_ref, kept_ref) = refs[:4], refs[4:6], refs[6:]
    for part in range(2):
        half = acts[2 * part : 2 * part + 2]
        at = slice(part * half[0].shape[0], (part + 1) * half[0].shape[0])
        other_ref[at, :] = down_part((1, 1, chips), *half, *weights)
        near_ref = near_b_ref if part else near_a_ref
        near_ref[...] = down_part((1, 0, chips), *half, *weights)
        kept_ref[at, :] = down_part((0, 0, chips), *half, *weights)


def sum_kernel(kept_ref, other_ref, near_a_ref, near_b_ref, out_ref):
    half = near_a_ref.shape[0]
    for part, near_ref in enumerate((near_a_ref, near_b_ref)):
        at = slice(part * half, (part + 1) * half)
        total = kept_ref[at, :].astype(jnp.float32) + other_ref[at, :].astype(jnp.float32)
        out_ref[at, :] = (total + near_ref[...].astype(jnp.float32)).astype(jnp.bfloat16)


def combine_kernel(share_ref, rows_ref, mix_ref, squares_ref):
    tokens = mix_ref.shape[0]
    parts = jnp.dot(share_ref[...], rows_ref[...], preferred_element_type=jnp.float32)
    mix = parts[:tokens] + parts[tokens : 2 * tokens] + parts[2 * tokens :]
    mix_ref[...] = mix
    ones = jnp.ones((8, mix.shape[1]), jnp.bfloat16)
    sums = functools.reduce(jnp.add, [dot_t(ones, part) for part in split3(mix * mix)])
    sums = jnp.concatenate([sums, jnp.zeros_like(sums)], axis=1)
    squares_ref[...] = sums


def final_kernel(model_width, mix_ref, squares_ref, around_ref, other_ref, gain_ref, out_ref):
    total = squares_ref[0:1, :] + around_ref[0:1, :] + other_ref[0:1, :]
    mix = mix_ref[...]
    tokens = mix.shape[0]
    wide = jnp.broadcast_to(total, (tokens, total.shape[1]))
    row = lax.broadcasted_iota(jnp.int32, wide.shape, 0)
    lane = lax.broadcasted_iota(jnp.int32, wide.shape, 1)
    column = jnp.sum(jnp.where(row == lane, wide, 0.0), axis=1, keepdims=True)
    scale = lax.rsqrt(column / model_width + EPSILON)
    out_ref[...] = (mix * scale * gain_ref[...]).astype(jnp.bfloat16)


def call(kernel, outs, *args, limit=8, flops=0, space=VMEM, scratch=()):
    single = not isinstance(outs, (list, tuple))
    if space is HBM:
        args = [pltpu.with_memory_space_constraint(arg, pltpu.HBM) for arg in args]
    return pl.pallas_call(
        kernel,
        out_shape=outs,
        in_specs=[space] * len(args),
        out_specs=VMEM if single else [VMEM] * len(outs),
        scratch_shapes=scratch,
        cost_estimate=pl.CostEstimate(flops=flops, bytes_accessed=0, transcendentals=0),
        compiler_params=pltpu.CompilerParams(vmem_limit_bytes=limit << 20),
    )(*args)


def shape_of(dims, dtype):
    return jax.ShapeDtypeStruct(dims, dtype)


def local(tokens, norm_gain, expert_ids, route_weights, gate_proj, up_proj, down_proj, final_gain):
    tok_rows, width = tokens.shape
    peers = lax.axis_size("tp")
    experts = lax.axis_size("ep")
    chips = peers // CORES
    capacity = min(tok_rows, 2 * tok_rows * expert_ids.shape[1] // experts)
    rows = experts * capacity
    model_width = width * peers

    def onward(value):
        pairs = [
            (y * CORES + c, ((y + 1 - 2 * c) % chips) * CORES + c)
            for y in range(chips)
            for c in range(CORES)
        ]
        return lax.ppermute(value, "tp", pairs)

    def opposite(value):
        last = CORES - 1
        pairs = [
            (y * CORES + last, ((y + chips // 2) % chips) * CORES + last) for y in range(chips)
        ]
        return lax.ppermute(value, "tp", pairs)

    def swap(value):
        pairs = [(y * CORES + c, y * CORES + 1 - c) for y in range(chips) for c in range(CORES)]
        return lax.ppermute(value, "tp", pairs)

    narrow = shape_of((rows, width), jnp.bfloat16)
    ids = expert_ids.T
    outbound, gain = call(
        functools.partial(pick_kernel, experts, capacity),
        [narrow, shape_of((1, width), jnp.float32)],
        ids,
        tokens,
        norm_gain[None, :],
        space=HBM,
        scratch=(
            pltpu.VMEM(ids.shape, jnp.int32),
            pltpu.VMEM(tokens.shape, jnp.bfloat16),
            pltpu.SemaphoreType.DMA((3,)),
        ),
    )
    received = lax.all_to_all(
        outbound.reshape(experts, capacity, width), "ep", split_axis=0, concat_axis=0, tiled=True
    ).reshape(rows, width)
    half = rows // 2
    whole, head, rest = [
        shape_of((n, width), jnp.bfloat16) for n in (rows + TAIL, half + TAIL, half)
    ]
    own, own_a, own_b = call(mid_kernel, [whole, head, rest], received, gain)

    first_a = onward(own_a)
    own_other = swap(own)
    first_b = onward(own_b)
    second = onward(own_other)
    third_a = onward(first_a)
    third_b = onward(first_b)
    first_other = (swap(first_a), swap(first_b))
    second_other = swap(second)
    third_other_a = swap(third_a)
    third_other_b = swap(third_b)
    sources = (ids, route_weights.T, final_gain[None, :], up_proj[0])
    share, final_gain, up = call(
        functools.partial(load_kernel, experts, capacity),
        [shape_of((3 * tok_rows, rows), jnp.bfloat16)]
        + [shape_of(source.shape, source.dtype) for source in sources[2:]],
        *sources,
        space=HBM,
        scratch=(
            pltpu.VMEM(ids.shape, jnp.int32),
            pltpu.VMEM(ids.shape, jnp.float32),
            pltpu.SemaphoreType.DMA((len(sources),)),
        ),
    )
    gate, down = gate_proj[0], down_proj[0]
    down_other = swap(down)
    early = [
        ((0, 0, chips), (own,)),
        ((0, 1, chips), (own_other,)),
        ((-1, 0, chips), (first_a, first_b)),
        ((1, 1, chips), first_other),
        ((-1, 1, chips), (second,)),
        ((1, 0, chips), (second_other,)),
    ]
    late = [(-2, 0, chips), (2, 1, chips)]
    wide = shape_of((rows, width), jnp.float32)
    flops = 4 * rows * width * width

    def sums_of(pieces, *before):
        return call(
            functools.partial(
                first_kernel, [where for where, _ in pieces], [len(held) for _, held in pieces]
            ),
            [wide, wide, shape_of((rows, 128), jnp.float32)],
            *[part for _, held in pieces for part in held],
            gate,
            up,
            *before,
            limit=16,
            flops=len(pieces) * flops,
        )

    sums = sums_of(early[4:], *sums_of(early[:4]))

    def last(part, *held):
        act = call(
            functools.partial(last_kernel, late, [len(held) // 2] * 2, part),
            rest,
            *held,
            gate,
            up,
            *sums,
            limit=16,
            flops=flops,
        )
        return act, swap(act)

    act_a = last(0, third_a, third_other_a)
    act_b = last(1, third_a, third_b, third_other_a, third_other_b)

    def far(acts):
        out = call(
            functools.partial(far_kernel, (2, 0, chips)),
            rest,
            *acts,
            down,
            down_other,
            limit=16,
            flops=flops // 2,
        )
        return onward(out)

    far_a = far(act_a)
    far_b = far(act_b)
    narrow = shape_of((rows, width), jnp.bfloat16)
    near_other, near_a, near_b, kept = call(
        functools.partial(rest_kernel, chips),
        [narrow, rest, rest, narrow],
        *act_a,
        *act_b,
        down,
        down_other,
        limit=16,
        flops=3 * flops,
    )
    near_other = onward(near_other)

    def near(mine, came):
        total = mine.astype(jnp.float32) + came.astype(jnp.float32)
        return onward(total.astype(jnp.bfloat16))

    near_a = near(near_a, far_a)
    near_b = near(near_b, far_b)
    near_other = swap(near_other)
    total = call(sum_kernel, narrow, kept, near_other, near_a, near_b)
    expert_out = total.reshape(experts, capacity, width)
    returned = lax.all_to_all(expert_out, "ep", split_axis=0, concat_axis=0, tiled=True)
    mixture, squares = call(
        combine_kernel,
        [shape_of((tok_rows, width), jnp.float32), shape_of((8, 128), jnp.float32)],
        share,
        returned.reshape(rows, width),
    )
    squares += swap(squares)
    across = opposite(squares)
    around = onward(squares) + across
    return call(
        functools.partial(final_kernel, model_width),
        shape_of((tok_rows, width), jnp.bfloat16),
        mixture,
        squares,
        around,
        swap(around),
        final_gain,
    )


def solution(mesh):
    placed = (
        P("ep", "tp"),
        P("tp"),
        P("ep", None),
        P("ep", None),
        P("ep", None, "tp"),
        P("ep", None, "tp"),
        P("ep", "tp", None),
        P("tp"),
    )

    return jax.shard_map(
        local, mesh=mesh, in_specs=placed, out_specs=P("ep", "tp"), check_vma=False
    )
```

```python
import functools

import jax
import jax.numpy as jnp
from jax import lax
from jax.experimental import pallas as pl
from jax.experimental.pallas import tpu as pltpu
from jax.sharding import PartitionSpec as P


EPSILON = 1e-05
CLAMP_LIMIT = 7.0
SIGMOID_SLOPE = 1.702
CORES = 2
TAIL = 16
VMEM = pl.BlockSpec(memory_space=pltpu.VMEM)
HBM = pl.BlockSpec(memory_space=pltpu.HBM)


def split3(v):
    hi = v.astype(jnp.bfloat16)
    rest = v - hi.astype(jnp.float32)
    mid = rest.astype(jnp.bfloat16)
    lo = (rest - mid.astype(jnp.float32)).astype(jnp.bfloat16)
    return hi, mid, lo


def dot_t(a, b):
    return lax.dot_general(a, b, (((1,), (1,)), ((), ())), preferred_element_type=jnp.float32)


def dot_0(a, b):
    return lax.dot_general(a, b, (((0,), (0,)), ((), ())), preferred_element_type=jnp.float32)


def slot_matrix(ids, experts, capacity):
    choices, tokens = ids.shape
    expert = lax.broadcasted_iota(jnp.int32, (experts, tokens), 0)
    named = [(ids[k : k + 1, :] == expert).astype(jnp.float32) for k in range(choices)]
    match = functools.reduce(jnp.add, named)
    before = lax.broadcasted_iota(jnp.int32, (tokens, tokens), 0)
    after = lax.broadcasted_iota(jnp.int32, (tokens, tokens), 1)
    earlier = (before < after).astype(jnp.bfloat16)
    place = jnp.dot(match.astype(jnp.bfloat16), earlier, preferred_element_type=jnp.float32)
    place = jnp.where(match > 0.0, place, -1.0)

    def spread(rows):
        wide = jnp.broadcast_to(rows[:, None, :], (experts, capacity, tokens))
        return wide.reshape(experts * capacity, tokens)

    slot = lax.broadcasted_iota(jnp.int32, (experts, capacity, tokens), 1)
    slot = slot.reshape(experts * capacity, tokens).astype(jnp.float32)
    holds = spread(place) == slot
    return holds, named, spread


def pick_kernel(experts, capacity, ids_hbm, tokens_hbm, gain_hbm, rows_ref, gain_ref, ids_ref, tokens_ref, sems):
    copies = [
        pltpu.make_async_copy(ids_hbm, ids_ref, sems.at[0]),
        pltpu.make_async_copy(tokens_hbm, tokens_ref, sems.at[1]),
        pltpu.make_async_copy(gain_hbm, gain_ref, sems.at[2]),
    ]
    for copy in copies:
        copy.start()
    copies[0].wait()
    holds, _, _ = slot_matrix(ids_ref[...], experts, capacity)
    holds = holds.astype(jnp.bfloat16)
    copies[1].wait()
    picked = jnp.dot(holds, tokens_ref[...], preferred_element_type=jnp.float32)
    rows_ref[...] = picked.astype(jnp.bfloat16)
    copies[2].wait()


def load_kernel(experts, capacity, *refs):
    *refs, ids_ref, weights_ref, sems = refs
    count = (len(refs) + 1) // 2
    ids_hbm, weights_hbm, *sources = refs[:count]
    share_ref, *targets = refs[count:]
    pairs = [(ids_hbm, ids_ref), (weights_hbm, weights_ref), *zip(sources, targets)]
    copies = [pltpu.make_async_copy(*pair, sems.at[i]) for i, pair in enumerate(pairs)]
    for copy in copies:
        copy.start()
    copies[0].wait()
    holds, named, spread = slot_matrix(ids_ref[...], experts, capacity)
    copies[1].wait()
    weights = weights_ref[...]
    share = functools.reduce(
        jnp.add, [weights[k : k + 1, :] * named[k] for k in range(len(named))]
    )
    share = jnp.where(holds, spread(share), 0.0).T
    tokens = share.shape[0]
    for i, part in enumerate(split3(share)):
        share_ref[i * tokens : (i + 1) * tokens, :] = part
    for copy in copies[2:]:
        copy.wait()


def mid_kernel(rows_ref, gain_ref, out_ref, out_a_ref, out_b_ref):
    rows, width = rows_ref.shape
    half = rows // 2
    x = rows_ref[...].astype(jnp.float32)
    scaled = (x * gain_ref[...]).astype(jnp.bfloat16)
    out_ref[0:rows, :] = scaled
    out_a_ref[0:half, :] = scaled[:half]
    out_b_ref[...] = scaled[half:]
    hi, mid, _ = split3(x * x)
    ones = jnp.ones((8, width), jnp.bfloat16)
    sums = dot_t(ones, hi) + dot_t(ones, mid)
    row = lax.broadcasted_iota(jnp.int32, (8, width), 0)
    tail = []
    for part in range(rows // width):
        pieces = [v.astype(jnp.float32) for v in split3(sums[:, part * width : (part + 1) * width])]
        tail.append(
            jnp.where(
                row == 0,
                pieces[0],
                jnp.where(row == 1, pieces[1], jnp.where(row == 2, pieces[2], 0.0)),
            )
        )
    tail = jnp.concatenate(tail, axis=0).astype(jnp.bfloat16)
    out_ref[rows : rows + TAIL, :] = tail
    out_a_ref[half : half + TAIL, :] = tail


def ahead(step, other, chips):
    me = lax.axis_index("tp")
    core = me % CORES
    return (me // CORES + step * (1 - 2 * core) + chips) % chips * CORES + (core + other) % CORES


def products(part, pieces, gate_ref, up_ref, gate, up, squares):
    width = gate_ref.shape[1]
    row = lax.broadcasted_iota(jnp.int32, (TAIL, 128), 0)
    ones = jnp.where(row // 8 == part, 1.0, 0.0).astype(jnp.bfloat16)
    for where, refs in pieces:
        from_row = pl.ds(pl.multiple_of(ahead(*where) * width, width), width)
        at = part * width if len(refs) == 1 else 0
        x = refs[part if len(refs) > 1 else 0][at : at + width, :]
        end = refs[0].shape[0]
        gate += jnp.dot(x, gate_ref[from_row, :], preferred_element_type=jnp.float32)
        up += jnp.dot(x, up_ref[from_row, :], preferred_element_type=jnp.float32)
        squares += dot_0(refs[0][end - TAIL : end, :], ones)
    return gate, up, squares


def grouped(places, sizes, refs):
    pieces, at = [], 0
    for where, size in zip(places, sizes):
        pieces.append((where, refs[at : at + size]))
        at += size
    return pieces, refs[at:]


def first_kernel(places, sizes, *refs):
    pieces, (gate_ref, up_ref, *before, gate_out, up_out, squares_out) = grouped(
        places, sizes, refs
    )
    width = gate_ref.shape[1]
    for part in range(gate_out.shape[0] // width):
        at = slice(part * width, (part + 1) * width)
        zero = jnp.zeros((width, width), jnp.float32)
        start = [ref[at, :] for ref in before] or [zero, zero, zero[:, :128]]
        gate, up, squares = products(part, pieces, gate_ref, up_ref, *start)
        gate_out[at, :] = gate
        up_out[at, :] = up
        squares_out[at, :] = squares


def last_kernel(places, sizes, part, *refs):
    pieces, refs = grouped(places, sizes, refs)
    gate_ref, up_ref, gate_in, up_in, squares_in, act_ref = refs
    model_width, width = gate_ref.shape
    at = slice(part * width, (part + 1) * width)
    gate, up, squares = products(
        part, pieces, gate_ref, up_ref, gate_in[at, :], up_in[at, :], squares_in[at, :]
    )
    scale = lax.rsqrt(squares / model_width + EPSILON)
    scale = jnp.concatenate([scale] * (width // 128), axis=1)
    gate = jnp.minimum(gate * scale, CLAMP_LIMIT)
    up = jnp.clip(up * scale, -CLAMP_LIMIT, CLAMP_LIMIT)
    act = (up + 1.0) * gate * jax.nn.sigmoid(SIGMOID_SLOPE * gate)
    act_ref[...] = act.astype(jnp.bfloat16)


def down_part(where, own_ref, other_ref, down_ref, down_other_ref):
    width = own_ref.shape[1]
    columns = pl.ds(pl.multiple_of(ahead(*where) * width, width), width)
    total = jnp.dot(own_ref[...], down_ref[:, columns], preferred_element_type=jnp.float32)
    total += jnp.dot(
        other_ref[...], down_other_ref[:, columns], preferred_element_type=jnp.float32
    )
    return total.astype(jnp.bfloat16)


def far_kernel(where, own_ref, other_ref, down_ref, down_other_ref, out_ref):
    out_ref[...] = down_part(where, own_ref, other_ref, down_ref, down_other_ref)


def rest_kernel(chips, *refs):
    acts, weights, (other_ref, near_a_ref, near_b_ref, kept_ref) = refs[:4], refs[4:6], refs[6:]
    for part in range(2):
        half = acts[2 * part : 2 * part + 2]
        at = slice(part * half[0].shape[0], (part + 1) * half[0].shape[0])
        other_ref[at, :] = down_part((1, 1, chips), *half, *weights)
        near_ref = near_b_ref if part else near_a_ref
        near_ref[...] = down_part((1, 0, chips), *half, *weights)
        kept_ref[at, :] = down_part((0, 0, chips), *half, *weights)


def sum_kernel(kept_ref, other_ref, near_a_ref, near_b_ref, out_ref):
    half = near_a_ref.shape[0]
    for part, near_ref in enumerate((near_a_ref, near_b_ref)):
        at = slice(part * half, (part + 1) * half)
        total = kept_ref[at, :].astype(jnp.float32) + other_ref[at, :].astype(jnp.float32)
        out_ref[at, :] = (total + near_ref[...].astype(jnp.float32)).astype(jnp.bfloat16)


def combine_kernel(share_ref, rows_ref, mix_ref, squares_ref):
    tokens = mix_ref.shape[0]
    parts = jnp.dot(share_ref[...], rows_ref[...], preferred_element_type=jnp.float32)
    mix = parts[:tokens] + parts[tokens : 2 * tokens] + parts[2 * tokens :]
    mix_ref[...] = mix
    ones = jnp.ones((8, mix.shape[1]), jnp.bfloat16)
    sums = functools.reduce(jnp.add, [dot_t(ones, part) for part in split3(mix * mix)])
    sums = jnp.concatenate([sums, jnp.zeros_like(sums)], axis=1)
    squares_ref[...] = sums


def final_kernel(model_width, mix_ref, *refs):
    *squares, gain_ref, out_ref = refs
    total = functools.reduce(jnp.add, [part[0:1, :] for part in squares])
    mix = mix_ref[...]
    tokens = mix.shape[0]
    wide = jnp.broadcast_to(total, (tokens, total.shape[1]))
    row = lax.broadcasted_iota(jnp.int32, wide.shape, 0)
    lane = lax.broadcasted_iota(jnp.int32, wide.shape, 1)
    column = jnp.sum(jnp.where(row == lane, wide, 0.0), axis=1, keepdims=True)
    scale = lax.rsqrt(column / model_width + EPSILON)
    out_ref[...] = (mix * scale * gain_ref[...]).astype(jnp.bfloat16)


def call(kernel, outs, *args, limit=8, flops=0, space=VMEM, scratch=()):
    single = not isinstance(outs, (list, tuple))
    if space is HBM:
        args = [pltpu.with_memory_space_constraint(arg, pltpu.HBM) for arg in args]
    return pl.pallas_call(
        kernel,
        out_shape=outs,
        in_specs=[space] * len(args),
        out_specs=VMEM if single else [VMEM] * len(outs),
        scratch_shapes=scratch,
        cost_estimate=pl.CostEstimate(flops=flops, bytes_accessed=0, transcendentals=0),
        compiler_params=pltpu.CompilerParams(vmem_limit_bytes=limit << 20),
    )(*args)


def shape_of(dims, dtype):
    return jax.ShapeDtypeStruct(dims, dtype)


def local(tokens, norm_gain, expert_ids, route_weights, gate_proj, up_proj, down_proj, final_gain):
    tok_rows, width = tokens.shape
    peers = lax.axis_size("tp")
    experts = lax.axis_size("ep")
    chips = peers // CORES
    capacity = min(tok_rows, 2 * tok_rows * expert_ids.shape[1] // experts)
    rows = experts * capacity
    model_width = width * peers

    def onward(value):
        pairs = [
            (y * CORES + c, ((y + 1 - 2 * c) % chips) * CORES + c)
            for y in range(chips)
            for c in range(CORES)
        ]
        return lax.ppermute(value, "tp", pairs)

    def opposite(value):
        pairs = [
            (y * CORES + c, ((y + chips // 2) % chips) * CORES + c)
            for y in range(chips)
            for c in range(CORES)
        ]
        return lax.ppermute(value, "tp", pairs)

    def swap(value):
        pairs = [(y * CORES + c, y * CORES + 1 - c) for y in range(chips) for c in range(CORES)]
        return lax.ppermute(value, "tp", pairs)

    narrow = shape_of((rows, width), jnp.bfloat16)
    ids = expert_ids.T
    outbound, gain = call(
        functools.partial(pick_kernel, experts, capacity),
        [narrow, shape_of((1, width), jnp.float32)],
        ids,
        tokens,
        norm_gain[None, :],
        space=HBM,
        scratch=(
            pltpu.VMEM(ids.shape, jnp.int32),
            pltpu.VMEM(tokens.shape, jnp.bfloat16),
            pltpu.SemaphoreType.DMA((3,)),
        ),
    )
    received = lax.all_to_all(
        outbound.reshape(experts, capacity, width), "ep", split_axis=0, concat_axis=0, tiled=True
    ).reshape(rows, width)
    half = rows // 2
    whole, head, rest = [
        shape_of((n, width), jnp.bfloat16) for n in (rows + TAIL, half + TAIL, half)
    ]
    own, own_a, own_b = call(mid_kernel, [whole, head, rest], received, gain)

    first_a = onward(own_a)
    own_other = swap(own)
    first_b = onward(own_b)
    second = onward(own_other)
    third_a = onward(first_a)
    third_b = onward(first_b)
    first_other = (swap(first_a), swap(first_b))
    second_other = swap(second)
    third_other_a = swap(third_a)
    third_other_b = swap(third_b)
    sources = (ids, route_weights.T, final_gain[None, :], up_proj[0])
    share, final_gain, up = call(
        functools.partial(load_kernel, experts, capacity),
        [shape_of((3 * tok_rows, rows), jnp.bfloat16)]
        + [shape_of(source.shape, source.dtype) for source in sources[2:]],
        *sources,
        space=HBM,
        scratch=(
            pltpu.VMEM(ids.shape, jnp.int32),
            pltpu.VMEM(ids.shape, jnp.float32),
            pltpu.SemaphoreType.DMA((len(sources),)),
        ),
    )
    gate, down = gate_proj[0], down_proj[0]
    down_other = swap(down)
    early = [
        ((0, 0, chips), (own,)),
        ((0, 1, chips), (own_other,)),
        ((-1, 0, chips), (first_a, first_b)),
        ((1, 1, chips), first_other),
        ((-1, 1, chips), (second,)),
        ((1, 0, chips), (second_other,)),
    ]
    late = [(-2, 0, chips), (2, 1, chips)]
    wide = shape_of((rows, width), jnp.float32)
    flops = 4 * rows * width * width

    def sums_of(pieces, *before):
        return call(
            functools.partial(
                first_kernel, [where for where, _ in pieces], [len(held) for _, held in pieces]
            ),
            [wide, wide, shape_of((rows, 128), jnp.float32)],
            *[part for _, held in pieces for part in held],
            gate,
            up,
            *before,
            limit=16,
            flops=len(pieces) * flops,
        )

    sums = sums_of(early[4:], *sums_of(early[:4]))

    def last(part, *held):
        act = call(
            functools.partial(last_kernel, late, [len(held) // 2] * 2, part),
            rest,
            *held,
            gate,
            up,
            *sums,
            limit=16,
            flops=flops,
        )
        return act, swap(act)

    act_a = last(0, third_a, third_other_a)
    act_b = last(1, third_a, third_b, third_other_a, third_other_b)

    def far(acts):
        out = call(
            functools.partial(far_kernel, (2, 0, chips)),
            rest,
            *acts,
            down,
            down_other,
            limit=16,
            flops=flops // 2,
        )
        return onward(out)

    far_a = far(act_a)
    far_b = far(act_b)
    narrow = shape_of((rows, width), jnp.bfloat16)
    near_other, near_a, near_b, kept = call(
        functools.partial(rest_kernel, chips),
        [narrow, rest, rest, narrow],
        *act_a,
        *act_b,
        down,
        down_other,
        limit=16,
        flops=3 * flops,
    )
    near_other = onward(near_other)

    def near(mine, came):
        total = mine.astype(jnp.float32) + came.astype(jnp.float32)
        return onward(total.astype(jnp.bfloat16))

    near_a = near(near_a, far_a)
    near_b = near(near_b, far_b)
    near_other = swap(near_other)
    total = call(sum_kernel, narrow, kept, near_other, near_a, near_b)
    expert_out = total.reshape(experts, capacity, width)
    returned = lax.all_to_all(expert_out, "ep", split_axis=0, concat_axis=0, tiled=True)
    mixture, squares = call(
        combine_kernel,
        [shape_of((tok_rows, width), jnp.float32), shape_of((8, 128), jnp.float32)],
        share,
        returned.reshape(rows, width),
    )
    squares += swap(squares)
    around = onward(squares)
    across = opposite(squares)
    return call(
        functools.partial(final_kernel, model_width),
        shape_of((tok_rows, width), jnp.bfloat16),
        mixture,
        squares,
        around,
        swap(around),
        across,
        final_gain,
    )


def solution(mesh):
    placed = (
        P("ep", "tp"),
        P("tp"),
        P("ep", None),
        P("ep", None),
        P("ep", None, "tp"),
        P("ep", None, "tp"),
        P("ep", "tp", None),
        P("tp"),
    )

    return jax.shard_map(
        local, mesh=mesh, in_specs=placed, out_specs=P("ep", "tp"), check_vma=False
    )
```

```python
import functools

import jax
import jax.numpy as jnp
from jax import lax
from jax.experimental import pallas as pl
from jax.experimental.pallas import tpu as pltpu
from jax.sharding import PartitionSpec as P


EPSILON = 1e-05
CLAMP_LIMIT = 7.0
SIGMOID_SLOPE = 1.702
CORES = 2
TAIL = 16
VMEM = pl.BlockSpec(memory_space=pltpu.VMEM)
HBM = pl.BlockSpec(memory_space=pltpu.HBM)


def split3(v):
    hi = v.astype(jnp.bfloat16)
    rest = v - hi.astype(jnp.float32)
    mid = rest.astype(jnp.bfloat16)
    lo = (rest - mid.astype(jnp.float32)).astype(jnp.bfloat16)
    return hi, mid, lo


def dot_t(a, b):
    return lax.dot_general(a, b, (((1,), (1,)), ((), ())), preferred_element_type=jnp.float32)


def dot_0(a, b):
    return lax.dot_general(a, b, (((0,), (0,)), ((), ())), preferred_element_type=jnp.float32)


def slot_matrix(ids, experts, capacity):
    choices, tokens = ids.shape
    expert = lax.broadcasted_iota(jnp.int32, (experts, tokens), 0)
    named = [(ids[k : k + 1, :] == expert).astype(jnp.float32) for k in range(choices)]
    match = functools.reduce(jnp.add, named)
    before = lax.broadcasted_iota(jnp.int32, (tokens, tokens), 0)
    after = lax.broadcasted_iota(jnp.int32, (tokens, tokens), 1)
    earlier = (before < after).astype(jnp.bfloat16)
    place = jnp.dot(match.astype(jnp.bfloat16), earlier, preferred_element_type=jnp.float32)
    place = jnp.where(match > 0.0, place, -1.0)

    def spread(rows):
        wide = jnp.broadcast_to(rows[:, None, :], (experts, capacity, tokens))
        return wide.reshape(experts * capacity, tokens)

    slot = lax.broadcasted_iota(jnp.int32, (experts, capacity, tokens), 1)
    slot = slot.reshape(experts * capacity, tokens).astype(jnp.float32)
    holds = spread(place) == slot
    return holds, named, spread


def pick_kernel(experts, capacity, ids_hbm, tokens_hbm, gain_hbm, rows_ref, gain_ref, ids_ref, tokens_ref, sems):
    copies = [
        pltpu.make_async_copy(ids_hbm, ids_ref, sems.at[0]),
        pltpu.make_async_copy(tokens_hbm, tokens_ref, sems.at[1]),
        pltpu.make_async_copy(gain_hbm, gain_ref, sems.at[2]),
    ]
    for copy in copies:
        copy.start()
    copies[0].wait()
    holds, _, _ = slot_matrix(ids_ref[...], experts, capacity)
    holds = holds.astype(jnp.bfloat16)
    copies[1].wait()
    picked = jnp.dot(holds, tokens_ref[...], preferred_element_type=jnp.float32)
    rows_ref[...] = picked.astype(jnp.bfloat16)
    copies[2].wait()


def load_kernel(experts, capacity, *refs):
    *refs, ids_ref, weights_ref, sems = refs
    count = (len(refs) + 1) // 2
    ids_hbm, weights_hbm, *sources = refs[:count]
    share_ref, *targets = refs[count:]
    pairs = [(ids_hbm, ids_ref), (weights_hbm, weights_ref), *zip(sources, targets)]
    copies = [pltpu.make_async_copy(*pair, sems.at[i]) for i, pair in enumerate(pairs)]
    for copy in copies:
        copy.start()
    copies[0].wait()
    holds, named, spread = slot_matrix(ids_ref[...], experts, capacity)
    copies[1].wait()
    weights = weights_ref[...]
    share = functools.reduce(
        jnp.add, [weights[k : k + 1, :] * named[k] for k in range(len(named))]
    )
    share = jnp.where(holds, spread(share), 0.0).T
    tokens = share.shape[0]
    for i, part in enumerate(split3(share)[:2]):
        share_ref[i * tokens : (i + 1) * tokens, :] = part
    for copy in copies[2:]:
        copy.wait()


def mid_kernel(rows_ref, gain_ref, out_ref, out_a_ref, out_b_ref):
    rows, width = rows_ref.shape
    half = rows // 2
    x = rows_ref[...].astype(jnp.float32)
    scaled = (x * gain_ref[...]).astype(jnp.bfloat16)
    out_ref[0:rows, :] = scaled
    out_a_ref[0:half, :] = scaled[:half]
    out_b_ref[...] = scaled[half:]
    hi, mid, _ = split3(x * x)
    ones = jnp.ones((8, width), jnp.bfloat16)
    sums = dot_t(ones, hi) + dot_t(ones, mid)
    row = lax.broadcasted_iota(jnp.int32, (8, width), 0)
    tail = []
    for part in range(rows // width):
        pieces = [v.astype(jnp.float32) for v in split3(sums[:, part * width : (part + 1) * width])]
        tail.append(
            jnp.where(
                row == 0,
                pieces[0],
                jnp.where(row == 1, pieces[1], jnp.where(row == 2, pieces[2], 0.0)),
            )
        )
    tail = jnp.concatenate(tail, axis=0).astype(jnp.bfloat16)
    out_ref[rows : rows + TAIL, :] = tail
    out_a_ref[half : half + TAIL, :] = tail


def ahead(step, other, chips):
    me = lax.axis_index("tp")
    core = me % CORES
    return (me // CORES + step * (1 - 2 * core) + chips) % chips * CORES + (core + other) % CORES


def products(part, pieces, gate_ref, up_ref, gate, up, squares):
    width = gate_ref.shape[1]
    row = lax.broadcasted_iota(jnp.int32, (TAIL, 128), 0)
    ones = jnp.where(row // 8 == part, 1.0, 0.0).astype(jnp.bfloat16)
    for where, refs in pieces:
        from_row = pl.ds(pl.multiple_of(ahead(*where) * width, width), width)
        at = part * width if len(refs) == 1 else 0
        x = refs[part if len(refs) > 1 else 0][at : at + width, :]
        end = refs[0].shape[0]
        gate += jnp.dot(x, gate_ref[from_row, :], preferred_element_type=jnp.float32)
        up += jnp.dot(x, up_ref[from_row, :], preferred_element_type=jnp.float32)
        squares += dot_0(refs[0][end - TAIL : end, :], ones)
    return gate, up, squares


def grouped(places, sizes, refs):
    pieces, at = [], 0
    for where, size in zip(places, sizes):
        pieces.append((where, refs[at : at + size]))
        at += size
    return pieces, refs[at:]


def first_kernel(places, sizes, *refs):
    pieces, (gate_ref, up_ref, *before, gate_out, up_out, squares_out) = grouped(
        places, sizes, refs
    )
    width = gate_ref.shape[1]
    for part in range(gate_out.shape[0] // width):
        at = slice(part * width, (part + 1) * width)
        zero = jnp.zeros((width, width), jnp.float32)
        start = [ref[at, :] for ref in before] or [zero, zero, zero[:, :128]]
        gate, up, squares = products(part, pieces, gate_ref, up_ref, *start)
        gate_out[at, :] = gate
        up_out[at, :] = up
        squares_out[at, :] = squares


def last_kernel(places, sizes, part, *refs):
    pieces, refs = grouped(places, sizes, refs)
    gate_ref, up_ref, gate_in, up_in, squares_in, act_ref = refs
    model_width, width = gate_ref.shape
    at = slice(part * width, (part + 1) * width)
    gate, up, squares = products(
        part, pieces, gate_ref, up_ref, gate_in[at, :], up_in[at, :], squares_in[at, :]
    )
    scale = lax.rsqrt(squares / model_width + EPSILON)
    scale = jnp.concatenate([scale] * (width // 128), axis=1)
    gate = jnp.minimum(gate * scale, CLAMP_LIMIT)
    up = jnp.clip(up * scale, -CLAMP_LIMIT, CLAMP_LIMIT)
    act = (up + 1.0) * gate * jax.nn.sigmoid(SIGMOID_SLOPE * gate)
    act_ref[...] = act.astype(jnp.bfloat16)


def down_part(where, own_ref, other_ref, down_ref, down_other_ref):
    width = own_ref.shape[1]
    columns = pl.ds(pl.multiple_of(ahead(*where) * width, width), width)
    total = jnp.dot(own_ref[...], down_ref[:, columns], preferred_element_type=jnp.float32)
    total += jnp.dot(
        other_ref[...], down_other_ref[:, columns], preferred_element_type=jnp.float32
    )
    return total.astype(jnp.bfloat16)


def far_kernel(where, own_ref, other_ref, down_ref, down_other_ref, out_ref):
    out_ref[...] = down_part(where, own_ref, other_ref, down_ref, down_other_ref)


def rest_kernel(chips, *refs):
    acts, weights, (other_ref, near_a_ref, near_b_ref, kept_ref) = refs[:4], refs[4:6], refs[6:]
    for part in range(2):
        half = acts[2 * part : 2 * part + 2]
        at = slice(part * half[0].shape[0], (part + 1) * half[0].shape[0])
        other_ref[at, :] = down_part((1, 1, chips), *half, *weights)
        near_ref = near_b_ref if part else near_a_ref
        near_ref[...] = down_part((1, 0, chips), *half, *weights)
        kept_ref[at, :] = down_part((0, 0, chips), *half, *weights)


def sum_kernel(kept_ref, other_ref, near_a_ref, near_b_ref, out_ref):
    half = near_a_ref.shape[0]
    for part, near_ref in enumerate((near_a_ref, near_b_ref)):
        at = slice(part * half, (part + 1) * half)
        total = kept_ref[at, :].astype(jnp.float32) + other_ref[at, :].astype(jnp.float32)
        out_ref[at, :] = (total + near_ref[...].astype(jnp.float32)).astype(jnp.bfloat16)


def combine_kernel(share_ref, rows_ref, mix_ref, squares_ref):
    tokens = mix_ref.shape[0]
    parts = jnp.dot(share_ref[...], rows_ref[...], preferred_element_type=jnp.float32)
    mix = parts[:tokens] + parts[tokens:]
    mix_ref[...] = mix
    ones = jnp.ones((8, mix.shape[1]), jnp.bfloat16)
    sums = functools.reduce(jnp.add, [dot_t(ones, part) for part in split3(mix * mix)[:2]])
    sums = jnp.concatenate([sums, jnp.zeros_like(sums)], axis=1)
    squares_ref[...] = sums


def final_kernel(model_width, mix_ref, *refs):
    *squares, gain_ref, out_ref = refs
    total = functools.reduce(jnp.add, [part[0:1, :] for part in squares])
    mix = mix_ref[...]
    tokens = mix.shape[0]
    wide = jnp.broadcast_to(total, (tokens, total.shape[1]))
    row = lax.broadcasted_iota(jnp.int32, wide.shape, 0)
    lane = lax.broadcasted_iota(jnp.int32, wide.shape, 1)
    column = jnp.sum(jnp.where(row == lane, wide, 0.0), axis=1, keepdims=True)
    scale = lax.rsqrt(column / model_width + EPSILON)
    out_ref[...] = (mix * scale * gain_ref[...]).astype(jnp.bfloat16)


def call(kernel, outs, *args, limit=8, flops=0, space=VMEM, scratch=()):
    single = not isinstance(outs, (list, tuple))
    if space is HBM:
        args = [pltpu.with_memory_space_constraint(arg, pltpu.HBM) for arg in args]
    return pl.pallas_call(
        kernel,
        out_shape=outs,
        in_specs=[space] * len(args),
        out_specs=VMEM if single else [VMEM] * len(outs),
        scratch_shapes=scratch,
        cost_estimate=pl.CostEstimate(flops=flops, bytes_accessed=0, transcendentals=0),
        compiler_params=pltpu.CompilerParams(vmem_limit_bytes=limit << 20),
    )(*args)


def shape_of(dims, dtype):
    return jax.ShapeDtypeStruct(dims, dtype)


def local(tokens, norm_gain, expert_ids, route_weights, gate_proj, up_proj, down_proj, final_gain):
    tok_rows, width = tokens.shape
    peers = lax.axis_size("tp")
    experts = lax.axis_size("ep")
    chips = peers // CORES
    capacity = min(tok_rows, 2 * tok_rows * expert_ids.shape[1] // experts)
    rows = experts * capacity
    model_width = width * peers

    def onward(value):
        pairs = [
            (y * CORES + c, ((y + 1 - 2 * c) % chips) * CORES + c)
            for y in range(chips)
            for c in range(CORES)
        ]
        return lax.ppermute(value, "tp", pairs)

    def opposite(value):
        pairs = [
            (y * CORES + c, ((y + chips // 2) % chips) * CORES + c)
            for y in range(chips)
            for c in range(CORES)
        ]
        return lax.ppermute(value, "tp", pairs)

    def swap(value):
        pairs = [(y * CORES + c, y * CORES + 1 - c) for y in range(chips) for c in range(CORES)]
        return lax.ppermute(value, "tp", pairs)

    narrow = shape_of((rows, width), jnp.bfloat16)
    ids = expert_ids.T
    outbound, gain = call(
        functools.partial(pick_kernel, experts, capacity),
        [narrow, shape_of((1, width), jnp.float32)],
        ids,
        tokens,
        norm_gain[None, :],
        space=HBM,
        scratch=(
            pltpu.VMEM(ids.shape, jnp.int32),
            pltpu.VMEM(tokens.shape, jnp.bfloat16),
            pltpu.SemaphoreType.DMA((3,)),
        ),
    )
    received = lax.all_to_all(
        outbound.reshape(experts, capacity, width), "ep", split_axis=0, concat_axis=0, tiled=True
    ).reshape(rows, width)
    half = rows // 2
    whole, head, rest = [
        shape_of((n, width), jnp.bfloat16) for n in (rows + TAIL, half + TAIL, half)
    ]
    own, own_a, own_b = call(mid_kernel, [whole, head, rest], received, gain)

    first_a = onward(own_a)
    own_other = swap(own)
    first_b = onward(own_b)
    second = onward(own_other)
    third_a = onward(first_a)
    third_b = onward(first_b)
    first_other = (swap(first_a), swap(first_b))
    second_other = swap(second)
    third_other_a = swap(third_a)
    third_other_b = swap(third_b)
    sources = (ids, route_weights.T, final_gain[None, :], up_proj[0])
    share, final_gain, up = call(
        functools.partial(load_kernel, experts, capacity),
        [shape_of((2 * tok_rows, rows), jnp.bfloat16)]
        + [shape_of(source.shape, source.dtype) for source in sources[2:]],
        *sources,
        space=HBM,
        scratch=(
            pltpu.VMEM(ids.shape, jnp.int32),
            pltpu.VMEM(ids.shape, jnp.float32),
            pltpu.SemaphoreType.DMA((len(sources),)),
        ),
    )
    gate, down = gate_proj[0], down_proj[0]
    down_other = swap(down)
    early = [
        ((0, 0, chips), (own,)),
        ((0, 1, chips), (own_other,)),
        ((-1, 0, chips), (first_a, first_b)),
        ((1, 1, chips), first_other),
        ((-1, 1, chips), (second,)),
        ((1, 0, chips), (second_other,)),
    ]
    late = [(-2, 0, chips), (2, 1, chips)]
    wide = shape_of((rows, width), jnp.float32)
    flops = 4 * rows * width * width

    def sums_of(pieces, *before):
        return call(
            functools.partial(
                first_kernel, [where for where, _ in pieces], [len(held) for _, held in pieces]
            ),
            [wide, wide, shape_of((rows, 128), jnp.float32)],
            *[part for _, held in pieces for part in held],
            gate,
            up,
            *before,
            limit=16,
            flops=len(pieces) * flops,
        )

    sums = sums_of(early[4:], *sums_of(early[:4]))

    def last(part, *held):
        act = call(
            functools.partial(last_kernel, late, [len(held) // 2] * 2, part),
            rest,
            *held,
            gate,
            up,
            *sums,
            limit=16,
            flops=flops,
        )
        return act, swap(act)

    act_a = last(0, third_a, third_other_a)
    act_b = last(1, third_a, third_b, third_other_a, third_other_b)

    def far(acts):
        out = call(
            functools.partial(far_kernel, (2, 0, chips)),
            rest,
            *acts,
            down,
            down_other,
            limit=16,
            flops=flops // 2,
        )
        return onward(out)

    far_a = far(act_a)
    far_b = far(act_b)
    narrow = shape_of((rows, width), jnp.bfloat16)
    near_other, near_a, near_b, kept = call(
        functools.partial(rest_kernel, chips),
        [narrow, rest, rest, narrow],
        *act_a,
        *act_b,
        down,
        down_other,
        limit=16,
        flops=3 * flops,
    )
    near_other = onward(near_other)

    def near(mine, came):
        total = mine.astype(jnp.float32) + came.astype(jnp.float32)
        return onward(total.astype(jnp.bfloat16))

    near_a = near(near_a, far_a)
    near_b = near(near_b, far_b)
    near_other = swap(near_other)
    total = call(sum_kernel, narrow, kept, near_other, near_a, near_b)
    expert_out = total.reshape(experts, capacity, width)
    returned = lax.all_to_all(expert_out, "ep", split_axis=0, concat_axis=0, tiled=True)
    mixture, squares = call(
        combine_kernel,
        [shape_of((tok_rows, width), jnp.float32), shape_of((8, 128), jnp.float32)],
        share,
        returned.reshape(rows, width),
    )
    squares += swap(squares)

    def beside(value, step):
        pairs = [
            (y * CORES + c, ((y + step) % chips) * CORES + c)
            for y in range(chips)
            for c in range(CORES)
        ]
        return lax.ppermute(value, "tp", pairs)

    around = beside(squares, 1)
    other_way = beside(squares, chips - 1)
    across = opposite(squares)
    return call(
        functools.partial(final_kernel, model_width),
        shape_of((tok_rows, width), jnp.bfloat16),
        mixture,
        squares,
        around,
        other_way,
        across,
        final_gain,
    )


def solution(mesh):
    placed = (
        P("ep", "tp"),
        P("tp"),
        P("ep", None),
        P("ep", None),
        P("ep", None, "tp"),
        P("ep", None, "tp"),
        P("ep", "tp", None),
        P("tp"),
    )

    return jax.shard_map(
        local, mesh=mesh, in_specs=placed, out_specs=P("ep", "tp"), check_vma=False
    )
```

```python
import functools

import jax
import jax.numpy as jnp
from jax import lax
from jax.experimental import pallas as pl
from jax.experimental.pallas import tpu as pltpu
from jax.sharding import PartitionSpec as P


EPSILON = 1e-05
CLAMP_LIMIT = 7.0
SIGMOID_SLOPE = 1.702
CORES = 2
TAIL = 16
VMEM = pl.BlockSpec(memory_space=pltpu.VMEM)
HBM = pl.BlockSpec(memory_space=pltpu.HBM)


def split3(v):
    hi = v.astype(jnp.bfloat16)
    rest = v - hi.astype(jnp.float32)
    mid = rest.astype(jnp.bfloat16)
    lo = (rest - mid.astype(jnp.float32)).astype(jnp.bfloat16)
    return hi, mid, lo


def dot_t(a, b):
    return lax.dot_general(a, b, (((1,), (1,)), ((), ())), preferred_element_type=jnp.float32)


def dot_0(a, b):
    return lax.dot_general(a, b, (((0,), (0,)), ((), ())), preferred_element_type=jnp.float32)


def slot_matrix(ids, experts, capacity):
    choices, tokens = ids.shape
    expert = lax.broadcasted_iota(jnp.int32, (experts, tokens), 0)
    named = [(ids[k : k + 1, :] == expert).astype(jnp.float32) for k in range(choices)]
    match = functools.reduce(jnp.add, named)
    before = lax.broadcasted_iota(jnp.int32, (tokens, tokens), 0)
    after = lax.broadcasted_iota(jnp.int32, (tokens, tokens), 1)
    earlier = (before < after).astype(jnp.bfloat16)
    place = jnp.dot(match.astype(jnp.bfloat16), earlier, preferred_element_type=jnp.float32)
    place = jnp.where(match > 0.0, place, -1.0)

    def spread(rows):
        wide = jnp.broadcast_to(rows[:, None, :], (experts, capacity, tokens))
        return wide.reshape(experts * capacity, tokens)

    slot = lax.broadcasted_iota(jnp.int32, (experts, capacity, tokens), 1)
    slot = slot.reshape(experts * capacity, tokens).astype(jnp.float32)
    holds = spread(place) == slot
    return holds, named, spread


def pick_kernel(experts, capacity, ids_hbm, tokens_hbm, gain_hbm, rows_ref, gain_ref, ids_ref, tokens_ref, sems):
    copies = [
        pltpu.make_async_copy(ids_hbm, ids_ref, sems.at[0]),
        pltpu.make_async_copy(tokens_hbm, tokens_ref, sems.at[1]),
        pltpu.make_async_copy(gain_hbm, gain_ref, sems.at[2]),
    ]
    for copy in copies:
        copy.start()
    copies[0].wait()
    holds, _, _ = slot_matrix(ids_ref[...], experts, capacity)
    holds = holds.astype(jnp.bfloat16)
    copies[1].wait()
    picked = jnp.dot(holds, tokens_ref[...], preferred_element_type=jnp.float32)
    rows_ref[...] = picked.astype(jnp.bfloat16)
    copies[2].wait()


def load_kernel(experts, capacity, *refs):
    *refs, ids_ref, weights_ref, sems = refs
    count = (len(refs) + 1) // 2
    ids_hbm, weights_hbm, *sources = refs[:count]
    share_ref, *targets = refs[count:]
    pairs = [(ids_hbm, ids_ref), (weights_hbm, weights_ref), *zip(sources, targets)]
    copies = [pltpu.make_async_copy(*pair, sems.at[i]) for i, pair in enumerate(pairs)]
    for copy in copies:
        copy.start()
    copies[0].wait()
    holds, named, spread = slot_matrix(ids_ref[...], experts, capacity)
    copies[1].wait()
    weights = weights_ref[...]
    share = functools.reduce(
        jnp.add, [weights[k : k + 1, :] * named[k] for k in range(len(named))]
    )
    share = jnp.where(holds, spread(share), 0.0).T
    tokens = share.shape[0]
    for i, part in enumerate(split3(share)[:2]):
        share_ref[i * tokens : (i + 1) * tokens, :] = part
    for copy in copies[2:]:
        copy.wait()


def mid_kernel(rows_ref, gain_ref, out_ref, out_a_ref, out_b_ref):
    rows, width = rows_ref.shape
    half = rows // 2
    x = rows_ref[...].astype(jnp.float32)
    scaled = (x * gain_ref[...]).astype(jnp.bfloat16)
    out_ref[0:rows, :] = scaled
    out_a_ref[0:half, :] = scaled[:half]
    out_b_ref[...] = scaled[half:]
    hi, mid, _ = split3(x * x)
    ones = jnp.ones((8, width), jnp.bfloat16)
    sums = dot_t(ones, hi) + dot_t(ones, mid)
    row = lax.broadcasted_iota(jnp.int32, (8, width), 0)
    tail = []
    for part in range(rows // width):
        pieces = [v.astype(jnp.float32) for v in split3(sums[:, part * width : (part + 1) * width])]
        tail.append(
            jnp.where(
                row == 0,
                pieces[0],
                jnp.where(row == 1, pieces[1], jnp.where(row == 2, pieces[2], 0.0)),
            )
        )
    tail = jnp.concatenate(tail, axis=0).astype(jnp.bfloat16)
    out_ref[rows : rows + TAIL, :] = tail
    out_a_ref[half : half + TAIL, :] = tail


def ahead(step, other, chips):
    me = lax.axis_index("tp")
    core = me % CORES
    return (me // CORES + step * (1 - 2 * core) + chips) % chips * CORES + (core + other) % CORES


def products(part, pieces, gate_ref, up_ref, gate, up, squares):
    width = gate_ref.shape[1]
    row = lax.broadcasted_iota(jnp.int32, (TAIL, 128), 0)
    ones = jnp.where(row // 8 == part, 1.0, 0.0).astype(jnp.bfloat16)
    for where, refs in pieces:
        from_row = pl.ds(pl.multiple_of(ahead(*where) * width, width), width)
        at = part * width if len(refs) == 1 else 0
        x = refs[part if len(refs) > 1 else 0][at : at + width, :]
        end = refs[0].shape[0]
        gate += jnp.dot(x, gate_ref[from_row, :], preferred_element_type=jnp.float32)
        up += jnp.dot(x, up_ref[from_row, :], preferred_element_type=jnp.float32)
        squares += dot_0(refs[0][end - TAIL : end, :], ones)
    return gate, up, squares


def grouped(places, sizes, refs):
    pieces, at = [], 0
    for where, size in zip(places, sizes):
        pieces.append((where, refs[at : at + size]))
        at += size
    return pieces, refs[at:]


def first_kernel(places, sizes, *refs):
    pieces, (gate_ref, up_ref, *before, gate_out, up_out, squares_out) = grouped(
        places, sizes, refs
    )
    width = gate_ref.shape[1]
    for part in range(gate_out.shape[0] // width):
        at = slice(part * width, (part + 1) * width)
        zero = jnp.zeros((width, width), jnp.float32)
        start = [ref[at, :] for ref in before] or [zero, zero, zero[:, :128]]
        gate, up, squares = products(part, pieces, gate_ref, up_ref, *start)
        gate_out[at, :] = gate
        up_out[at, :] = up
        squares_out[at, :] = squares


def last_kernel(places, sizes, part, *refs):
    pieces, refs = grouped(places, sizes, refs)
    gate_ref, up_ref, gate_in, up_in, squares_in, act_ref = refs
    model_width, width = gate_ref.shape
    at = slice(part * width, (part + 1) * width)
    gate, up, squares = products(
        part, pieces, gate_ref, up_ref, gate_in[at, :], up_in[at, :], squares_in[at, :]
    )
    scale = lax.rsqrt(squares / model_width + EPSILON)
    scale = jnp.concatenate([scale] * (width // 128), axis=1)
    gate = jnp.minimum(gate * scale, CLAMP_LIMIT)
    up = jnp.clip(up * scale, -CLAMP_LIMIT, CLAMP_LIMIT)
    act = (up + 1.0) * gate * jax.nn.sigmoid(SIGMOID_SLOPE * gate)
    act_ref[...] = act.astype(jnp.bfloat16)


def down_part(where, own_ref, other_ref, down_ref, down_other_ref):
    width = own_ref.shape[1]
    columns = pl.ds(pl.multiple_of(ahead(*where) * width, width), width)
    total = jnp.dot(own_ref[...], down_ref[:, columns], preferred_element_type=jnp.float32)
    total += jnp.dot(
        other_ref[...], down_other_ref[:, columns], preferred_element_type=jnp.float32
    )
    return total.astype(jnp.bfloat16)


def far_kernel(where, own_ref, other_ref, down_ref, down_other_ref, out_ref):
    out_ref[...] = down_part(where, own_ref, other_ref, down_ref, down_other_ref)


def rest_kernel(chips, *refs):
    acts, weights, (other_ref, near_a_ref, near_b_ref, kept_ref) = refs[:4], refs[4:6], refs[6:]
    for part in range(2):
        half = acts[2 * part : 2 * part + 2]
        at = slice(part * half[0].shape[0], (part + 1) * half[0].shape[0])
        other_ref[at, :] = down_part((1, 1, chips), *half, *weights)
        near_ref = near_b_ref if part else near_a_ref
        near_ref[...] = down_part((1, 0, chips), *half, *weights)
        kept_ref[at, :] = down_part((0, 0, chips), *half, *weights)


def sum_kernel(kept_ref, other_ref, near_a_ref, near_b_ref, out_ref):
    half = near_a_ref.shape[0]
    for part, near_ref in enumerate((near_a_ref, near_b_ref)):
        at = slice(part * half, (part + 1) * half)
        total = kept_ref[at, :].astype(jnp.float32) + other_ref[at, :].astype(jnp.float32)
        out_ref[at, :] = (total + near_ref[...].astype(jnp.float32)).astype(jnp.bfloat16)


def combine_kernel(share_ref, rows_ref, mix_ref, squares_ref):
    tokens = mix_ref.shape[0]
    parts = jnp.dot(share_ref[...], rows_ref[...], preferred_element_type=jnp.float32)
    mix = parts[:tokens] + parts[tokens:]
    mix_ref[...] = mix
    ones = jnp.ones((8, mix.shape[1]), jnp.bfloat16)
    sums = functools.reduce(jnp.add, [dot_t(ones, part) for part in split3(mix * mix)[:2]])
    sums = jnp.concatenate([sums, jnp.zeros_like(sums)], axis=1)
    squares_ref[...] = sums


def final_kernel(model_width, mix_ref, *refs):
    *squares, gain_ref, out_ref = refs
    total = functools.reduce(jnp.add, [part[0:1, :] for part in squares])
    mix = mix_ref[...]
    tokens = mix.shape[0]
    wide = jnp.broadcast_to(total, (tokens, total.shape[1]))
    row = lax.broadcasted_iota(jnp.int32, wide.shape, 0)
    lane = lax.broadcasted_iota(jnp.int32, wide.shape, 1)
    column = jnp.sum(jnp.where(row == lane, wide, 0.0), axis=1, keepdims=True)
    scale = lax.rsqrt(column / model_width + EPSILON)
    out_ref[...] = (mix * scale * gain_ref[...]).astype(jnp.bfloat16)


def call(kernel, outs, *args, limit=8, flops=0, space=VMEM, scratch=()):
    single = not isinstance(outs, (list, tuple))
    if space is HBM:
        args = [pltpu.with_memory_space_constraint(arg, pltpu.HBM) for arg in args]
    return pl.pallas_call(
        kernel,
        out_shape=outs,
        in_specs=[space] * len(args),
        out_specs=VMEM if single else [VMEM] * len(outs),
        scratch_shapes=scratch,
        cost_estimate=pl.CostEstimate(flops=flops, bytes_accessed=0, transcendentals=0),
        compiler_params=pltpu.CompilerParams(vmem_limit_bytes=limit << 20),
    )(*args)


def shape_of(dims, dtype):
    return jax.ShapeDtypeStruct(dims, dtype)


def local(tokens, norm_gain, expert_ids, route_weights, gate_proj, up_proj, down_proj, final_gain):
    tok_rows, width = tokens.shape
    peers = lax.axis_size("tp")
    experts = lax.axis_size("ep")
    chips = peers // CORES
    capacity = min(tok_rows, 2 * tok_rows * expert_ids.shape[1] // experts)
    rows = experts * capacity
    model_width = width * peers

    def onward(value):
        pairs = [
            (y * CORES + c, ((y + 1 - 2 * c) % chips) * CORES + c)
            for y in range(chips)
            for c in range(CORES)
        ]
        return lax.ppermute(value, "tp", pairs)

    def opposite(value):
        pairs = [
            (y * CORES + c, ((y + chips // 2) % chips) * CORES + c)
            for y in range(chips)
            for c in range(CORES)
        ]
        return lax.ppermute(value, "tp", pairs)

    def swap(value):
        pairs = [(y * CORES + c, y * CORES + 1 - c) for y in range(chips) for c in range(CORES)]
        return lax.ppermute(value, "tp", pairs)

    narrow = shape_of((rows, width), jnp.bfloat16)
    ids = expert_ids.T
    outbound, gain = call(
        functools.partial(pick_kernel, experts, capacity),
        [narrow, shape_of((1, width), jnp.float32)],
        ids,
        tokens,
        norm_gain[None, :],
        space=HBM,
        scratch=(
            pltpu.VMEM(ids.shape, jnp.int32),
            pltpu.VMEM(tokens.shape, jnp.bfloat16),
            pltpu.SemaphoreType.DMA((3,)),
        ),
    )
    received = lax.all_to_all(
        outbound.reshape(experts, capacity, width), "ep", split_axis=0, concat_axis=0, tiled=True
    ).reshape(rows, width)
    half = rows // 2
    whole, head, rest = [
        shape_of((n, width), jnp.bfloat16) for n in (rows + TAIL, half + TAIL, half)
    ]
    own, own_a, own_b = call(mid_kernel, [whole, head, rest], received, gain)

    first_a = onward(own_a)
    own_other = swap(own)
    first_b = onward(own_b)
    second = onward(own_other)
    third_a = onward(first_a)
    third_b = onward(first_b)
    first_other = (swap(first_a), swap(first_b))
    second_other = swap(second)
    third_other_a = swap(third_a)
    third_other_b = swap(third_b)
    sources = (ids, route_weights.T, final_gain[None, :], up_proj[0], gate_proj[0])
    share, final_gain, up, gate = call(
        functools.partial(load_kernel, experts, capacity),
        [shape_of((2 * tok_rows, rows), jnp.bfloat16)]
        + [shape_of(source.shape, source.dtype) for source in sources[2:]],
        *sources,
        space=HBM,
        scratch=(
            pltpu.VMEM(ids.shape, jnp.int32),
            pltpu.VMEM(ids.shape, jnp.float32),
            pltpu.SemaphoreType.DMA((len(sources),)),
        ),
    )
    down = down_proj[0]
    down_other = swap(down)
    early = [
        ((0, 0, chips), (own,)),
        ((0, 1, chips), (own_other,)),
        ((-1, 0, chips), (first_a, first_b)),
        ((1, 1, chips), first_other),
        ((-1, 1, chips), (second,)),
        ((1, 0, chips), (second_other,)),
    ]
    late = [(-2, 0, chips), (2, 1, chips)]
    wide = shape_of((rows, width), jnp.float32)
    flops = 4 * rows * width * width

    def sums_of(pieces, *before):
        return call(
            functools.partial(
                first_kernel, [where for where, _ in pieces], [len(held) for _, held in pieces]
            ),
            [wide, wide, shape_of((rows, 128), jnp.float32)],
            *[part for _, held in pieces for part in held],
            gate,
            up,
            *before,
            limit=16,
            flops=len(pieces) * flops,
        )

    sums = sums_of(early[4:], *sums_of(early[:4]))

    def last(part, *held):
        act = call(
            functools.partial(last_kernel, late, [len(held) // 2] * 2, part),
            rest,
            *held,
            gate,
            up,
            *sums,
            limit=16,
            flops=flops,
        )
        return act, swap(act)

    act_a = last(0, third_a, third_other_a)
    act_b = last(1, third_a, third_b, third_other_a, third_other_b)

    def far(acts):
        out = call(
            functools.partial(far_kernel, (2, 0, chips)),
            rest,
            *acts,
            down,
            down_other,
            limit=16,
            flops=flops // 2,
        )
        return onward(out)

    far_a = far(act_a)
    far_b = far(act_b)
    narrow = shape_of((rows, width), jnp.bfloat16)
    near_other, near_a, near_b, kept = call(
        functools.partial(rest_kernel, chips),
        [narrow, rest, rest, narrow],
        *act_a,
        *act_b,
        down,
        down_other,
        limit=16,
        flops=3 * flops,
    )
    near_other = onward(near_other)

    def near(mine, came):
        total = mine.astype(jnp.float32) + came.astype(jnp.float32)
        return onward(total.astype(jnp.bfloat16))

    near_a = near(near_a, far_a)
    near_b = near(near_b, far_b)
    near_other = swap(near_other)
    total = call(sum_kernel, narrow, kept, near_other, near_a, near_b)
    expert_out = total.reshape(experts, capacity, width)
    returned = lax.all_to_all(expert_out, "ep", split_axis=0, concat_axis=0, tiled=True)
    mixture, squares = call(
        combine_kernel,
        [shape_of((tok_rows, width), jnp.float32), shape_of((8, 128), jnp.float32)],
        share,
        returned.reshape(rows, width),
    )
    squares += swap(squares)

    def beside(value, step):
        pairs = [
            (y * CORES + c, ((y + step) % chips) * CORES + c)
            for y in range(chips)
            for c in range(CORES)
        ]
        return lax.ppermute(value, "tp", pairs)

    around = beside(squares, 1)
    other_way = beside(squares, chips - 1)
    across = opposite(squares)
    return call(
        functools.partial(final_kernel, model_width),
        shape_of((tok_rows, width), jnp.bfloat16),
        mixture,
        squares,
        around,
        other_way,
        across,
        final_gain,
    )


def solution(mesh):
    placed = (
        P("ep", "tp"),
        P("tp"),
        P("ep", None),
        P("ep", None),
        P("ep", None, "tp"),
        P("ep", None, "tp"),
        P("ep", "tp", None),
        P("tp"),
    )

    return jax.shard_map(
        local, mesh=mesh, in_specs=placed, out_specs=P("ep", "tp"), check_vma=False
    )
```
